256 devices in a mesh: sp: 32 (over z, y), fs: 4 (over x), tp: 2 (over core).
Axes of the slice: x: 4, y: 4, z: 8, core: 2. Of those that a mesh axis runs over, the one named last changes fastest.
Arguments:
- tokens: bfloat16 [8, 6144, 2048], P(('fs', 'tp'), 'sp'), may hold values from -6 to 6
- linear_query: bfloat16 [2048, 512], P(('sp', 'tp'), 'fs'), may hold values from -0.125 to 0.125
- linear_key: bfloat16 [2048, 512], P(('sp', 'tp'), 'fs'), may hold values from -0.125 to 0.125
- linear_decay: bfloat16 [2048, 512], P(('sp', 'tp'), 'fs'), may hold values from -0.25 to 0.25
- linear_value: bfloat16 [2048, 1024], P(('sp', 'tp'), 'fs'), may hold values from -0.125 to 0.125
- linear_gate: bfloat16 [2048, 1024], P(('sp', 'tp'), 'fs'), may hold values from -0.125 to 0.125
- decay_bias: float32 [512], P('fs'), may hold values from 2 to 5.5
- norm_gain: float32 [256], replicated, may hold values from 0.1 to 1.9
- window_query: bfloat16 [2048, 1024], P(('sp', 'tp'), 'fs'), may hold values from -0.125 to 0.125
- window_key: bfloat16 [2048, 256], P(('sp', 'tp'), 'fs'), may hold values from -0.125 to 0.125
- window_value: bfloat16 [2048, 256], P(('sp', 'tp'), 'fs'), may hold values from -0.5 to 0.5
- sink_logit: float32 [16], P('fs'), may hold values from 3 to 7
- linear_output: bfloat16 [1024, 2048], P('fs'), may hold values from -0.1875 to 0.1875
- window_output: bfloat16 [1024, 2048], P('fs'), may hold values from -0.1875 to 0.1875
Outputs:
- mixed: bfloat16 [8, 6144, 2048], P(('fs', 'tp'), 'sp')
The draws below stay inside these ranges and needn't reach their ends.
All inputs are finite; a program needn't handle non-finite values.
Results may differ from the reference program's by a relative error of at most 0.025.
Values may be sent and summed in bfloat16 or wider, within the bound.
A program may use at most 64 MiB of HBM per device.

```python
import jax
import jax.numpy as jnp
from jax import lax

D = 2048
GLA_HEADS = 4
GLA_KEY = 128
GLA_VALUE = 256
SWA_HEADS = 16
KV_HEADS = 4
HEAD_DIM = 64
WINDOW = 128
BLOCK = 32
SEQ = 6144
BATCH = 8
GATE_TAU = 384


def shard_levels(own_key, dims, pieces, least, high):
    loudness = 1.0
    for dim, shards_of in pieces:
        heights = jax.random.uniform(jax.random.fold_in(jax.random.fold_in(own_key, 6), dim), (shards_of,), jnp.float32, least / len(pieces), high / len(pieces))
        loudness = loudness * jnp.repeat(jnp.exp(heights), dims[dim] // shards_of).reshape((-1,) + (1,) * (len(dims) - 1 - dim))
    return loudness


def bell_draw(own_key, shape, scale, most, cuts=(), kind=jnp.bfloat16):
    result = scale * jax.random.normal(own_key, shape, jnp.float32)
    if cuts:
        result = result * shard_levels(own_key, shape, cuts, -0.22, 0.18)
    return jnp.clip(result, -most, most).astype(kind)


def setup_inputs(seed: int = 0) -> dict:
    arg_keys = jax.random.split(jax.random.key(seed), 15)
    return {
        "tokens": bell_draw(arg_keys[0], (BATCH, SEQ, D), 1.0, 6.0, ((0, 8), (1, 32))),
        "linear_query": bell_draw(arg_keys[1], (D, GLA_HEADS * GLA_KEY), D ** -0.5, 0.125, ((0, 64), (1, 4))),
        "linear_key": bell_draw(arg_keys[2], (D, GLA_HEADS * GLA_KEY), D ** -0.5, 0.125, ((0, 64), (1, 4))),
        "linear_decay": bell_draw(arg_keys[3], (D, GLA_HEADS * GLA_KEY), (D // 4) ** -0.5, 0.25, ((0, 64), (1, 4))),
        "linear_value": bell_draw(arg_keys[4], (D, GLA_HEADS * GLA_VALUE), D ** -0.5, 0.125, ((0, 64), (1, 4))),
        "linear_gate": bell_draw(arg_keys[5], (D, GLA_HEADS * GLA_VALUE), D ** -0.5, 0.125, ((0, 64), (1, 4))),
        "decay_bias": jnp.clip(2.0 + 3.5 * jax.random.uniform(arg_keys[6], (GLA_HEADS * GLA_KEY,), jnp.float32) ** shard_levels(arg_keys[6], (GLA_HEADS * GLA_KEY,), ((0, 4),), -0.2, 0.2), 2.0, 5.5),
        "norm_gain": jnp.clip(1.0 + 0.18 * jax.random.normal(arg_keys[7], (GLA_VALUE,), jnp.float32), 0.1, 1.9),
        "window_query": bell_draw(arg_keys[8], (D, SWA_HEADS * HEAD_DIM), D ** -0.5, 0.125, ((0, 64), (1, 4))),
        "window_key": bell_draw(arg_keys[9], (D, KV_HEADS * HEAD_DIM), D ** -0.5, 0.125, ((0, 64), (1, 4))),
        "window_value": bell_draw(arg_keys[10], (D, KV_HEADS * HEAD_DIM), (D // 16) ** -0.5, 0.5, ((0, 64), (1, 4))),
        "sink_logit": jnp.clip(3.0 + 4.0 * jax.random.uniform(arg_keys[11], (SWA_HEADS,), jnp.float32) ** shard_levels(arg_keys[11], (SWA_HEADS,), ((0, 4),), -0.2, 0.2), 3.0, 7.0),
        "linear_output": bell_draw(arg_keys[12], (GLA_HEADS * GLA_VALUE, D), (GLA_HEADS * GLA_VALUE) ** -0.5, 0.1875, ((0, 4),)),
        "window_output": bell_draw(arg_keys[13], (SWA_HEADS * HEAD_DIM, D), (SWA_HEADS * HEAD_DIM) ** -0.5, 0.1875, ((0, 4),)),
    }


norm_epsilon = 1e-05
highest = lax.Precision.HIGHEST

def project(inputs, weight):
    flat_rows = inputs.reshape(-1, inputs.shape[-1])
    product = jnp.dot(flat_rows, weight, preferred_element_type=jnp.float32).astype(jnp.bfloat16)
    return product.reshape(inputs.shape[:-1] + (weight.shape[1],))

def forget_blocks(queries, key_rows, value_rows, forget_logs, block_len):
    batch_size, length, head_count, key_dim = queries.shape
    value_dim = value_rows.shape[-1]
    block_count = length // block_len

    def to_blocks(tensor):
        return tensor.reshape(batch_size, block_count, block_len, head_count, tensor.shape[-1]).transpose(1, 0, 3, 2, 4)

    def from_blocks(tensor):
        return tensor.transpose(1, 0, 3, 2, 4).reshape(batch_size, length, head_count, tensor.shape[-1])
    causal = jnp.tril(jnp.ones((block_len, block_len), dtype=bool))

    def advance(carry, block_inputs):
        carry_state, offset = carry
        query_blk, key_blk, value_blk, forget_blk = block_inputs
        within = jnp.cumsum(forget_blk, axis=2)
        carried = jnp.einsum('bhcd,bhde->bhce', query_blk * jnp.exp(within), carry_state, precision=highest)
        spread = within[:, :, :, None, :] - within[:, :, None, :, :]
        decays = jnp.exp(jnp.where(causal[:, :, None], spread, -jnp.inf))
        scores = jnp.einsum('bhijd,bhjd->bhij', query_blk[:, :, :, None, :] * decays, key_blk, precision=highest)
        inside = jnp.einsum('bhij,bhje->bhie', scores, value_blk, precision=highest)
        final_log = within[:, :, -1, :]
        faded = key_blk * jnp.exp(final_log[:, :, None, :] - within)
        new_state = carry_state * jnp.exp(final_log)[:, :, :, None] + jnp.einsum('bhcd,bhce->bhde', faded, value_blk, precision=highest)
        reaching = jnp.exp(offset[:, :, None, :] + within)
        return ((new_state, offset + final_log), (carried + inside, reaching))
    zero_state = jnp.zeros((batch_size, head_count, key_dim, value_dim), jnp.float32)
    zero_offset = jnp.zeros((batch_size, head_count, key_dim), jnp.float32)
    blocked = (to_blocks(queries), to_blocks(key_rows), to_blocks(value_rows), to_blocks(forget_logs))
    finals, produced = lax.scan(advance, (zero_state, zero_offset), blocked)
    return (from_blocks(produced[0]), from_blocks(produced[1]), finals[0], finals[1])

def finish_linear(state_rows, gate_rows, norm_gain):
    scaled = state_rows * lax.rsqrt(lax.optimization_barrier(jnp.mean(jnp.square(state_rows), axis=-1, keepdims=True)) + norm_epsilon)
    gated = scaled * norm_gain.astype(jnp.float32) * jax.nn.silu(gate_rows.astype(jnp.float32))
    return gated.reshape(state_rows.shape[0], state_rows.shape[1], -1).astype(jnp.bfloat16)

def window_attend(queries, key_rows, value_rows, sink_logit, query_first, window_len, block_len):
    batch_size, length, query_heads, head_dim = queries.shape
    prior_rows = key_rows.shape[1] - length
    kv_heads = key_rows.shape[2]
    group_size = query_heads // kv_heads
    block_count = length // block_len
    span_len = window_len + block_len
    grouped = queries.reshape(batch_size, block_count, block_len, kv_heads, group_size, head_dim)
    sink_grid = sink_logit.astype(jnp.float32).reshape(kv_heads, group_size)[None, :, :, None, None]

    def attend(block_number):
        query_blk = lax.dynamic_index_in_dim(grouped, block_number, 1, keepdims=False)
        start_row = block_number * block_len + prior_rows - window_len
        key_blk = lax.dynamic_slice_in_dim(key_rows, start_row, span_len, 1)
        value_blk = lax.dynamic_slice_in_dim(value_rows, start_row, span_len, 1)
        scores = jnp.einsum('bqhgd,bkhd->bhgqk', query_blk, key_blk, precision=highest) * head_dim ** (-0.5)
        query_pos = query_first + block_number * block_len + jnp.arange(block_len, dtype=jnp.int32)
        key_pos = query_first - prior_rows + start_row + jnp.arange(span_len, dtype=jnp.int32)
        distance = query_pos[:, None] - key_pos[None, :]
        allowed = (distance >= 0) & (distance < window_len) & (key_pos[None, :] >= 0)
        scores = jnp.where(allowed, scores, -jnp.inf)
        highest_score = jnp.maximum(lax.optimization_barrier(jnp.max(scores, axis=-1, keepdims=True)), sink_grid)
        weights = jnp.exp(scores - highest_score)
        normaliser = lax.optimization_barrier(jnp.sum(weights, axis=-1, keepdims=True)) + jnp.exp(sink_grid - highest_score)
        return jnp.einsum('bhgqk,bkhd->bqhgd', weights / normaliser, value_blk, precision=highest)
    blocks_out = lax.map(attend, jnp.arange(block_count, dtype=jnp.int32))
    return blocks_out.transpose(1, 0, 2, 3, 4, 5).reshape(batch_size, length, query_heads * head_dim)

def reference(tokens, linear_query, linear_key, linear_decay, linear_value, linear_gate, decay_bias, norm_gain, window_query, window_key, window_value, sink_logit, linear_output, window_output):
    batch_size, length = (tokens.shape[0], tokens.shape[1])
    state_query = project(tokens, linear_query).astype(jnp.float32).reshape(batch_size, length, GLA_HEADS, GLA_KEY) * GLA_KEY ** (-0.5)
    state_key = project(tokens, linear_key).astype(jnp.float32).reshape(batch_size, length, GLA_HEADS, GLA_KEY)
    decay_input = project(tokens, linear_decay).astype(jnp.float32).reshape(batch_size, length, GLA_HEADS, GLA_KEY)
    state_value = project(tokens, linear_value).astype(jnp.float32).reshape(batch_size, length, GLA_HEADS, GLA_VALUE)
    state_gate = project(tokens, linear_gate).reshape(batch_size, length, GLA_HEADS, GLA_VALUE)
    forget_logs = jax.nn.log_sigmoid(decay_input + decay_bias.astype(jnp.float32).reshape(GLA_HEADS, GLA_KEY)) / GATE_TAU
    state_rows = forget_blocks(state_query, state_key, state_value, forget_logs, BLOCK)[0]
    linear_rows = finish_linear(state_rows, state_gate, norm_gain)
    local_query = project(tokens, window_query).astype(jnp.float32).reshape(batch_size, length, SWA_HEADS, HEAD_DIM)
    local_key = project(tokens, window_key).astype(jnp.float32).reshape(batch_size, length, KV_HEADS, HEAD_DIM)
    local_value = project(tokens, window_value).astype(jnp.float32).reshape(batch_size, length, KV_HEADS, HEAD_DIM)
    padding = ((0, 0), (WINDOW, 0), (0, 0), (0, 0))
    padded_keys = jnp.pad(local_key, padding)
    padded_values = jnp.pad(local_value, padding)
    window_rows = window_attend(local_query, padded_keys, padded_values, sink_logit, 0, WINDOW, BLOCK).astype(jnp.bfloat16)
    linear_part = jnp.dot(linear_rows.reshape(-1, GLA_HEADS * GLA_VALUE), linear_output, preferred_element_type=jnp.float32)
    window_part = jnp.dot(window_rows.reshape(-1, SWA_HEADS * HEAD_DIM), window_output, preferred_element_type=jnp.float32)
    mixed = (linear_part + window_part).astype(jnp.bfloat16)
    return mixed.reshape(batch_size, length, D)
```

```python
import functools

import jax
import jax.numpy as jnp
from jax import lax
from jax.experimental import pallas as pl
from jax.experimental.pallas import tpu as pltpu
from jax.sharding import PartitionSpec as P

GLA_KEY = 128
GLA_VALUE = 256
HEAD_DIM = 64
WINDOW = 128
NY = 4

norm_epsilon = 1e-05
MESH = pl.DeviceIdType.MESH
f32, bf16 = jnp.float32, jnp.bfloat16


def dot(a, b):
    return jnp.dot(a, b, preferred_element_type=f32)


def dot_t(a, b):
    return lax.dot_general(a, b, (((1,), (1,)), ((), ())), preferred_element_type=f32)


def dot_rows(a, b):
    return lax.dot_general(a, b, (((0,), (0,)), ((), ())), preferred_element_type=f32)


def kernel(
    NS, NF, NT, levels,
    tok, w_decay, w_key, w_value, w_wq, w_lq, w_gate, lin_o, win_o, w_wk, w_wv, bias, gain, sink,
    out,
    toks, W1, W2, out_w, sums, f2, kkey, val, kvbuf, lst, arr, pre, state_in, rows, oacc, reach, gates, part, rbuf,
    lsem, zs, zr, ys, yr, rs, rr, dsnd, drcv, ts, tr, hs, hr, asnd, arcv, qs, qr, ps, pr,
):
    sp, f, t = lax.axis_index("sp"), lax.axis_index("fs"), lax.axis_index("tp")
    NZ = NS // NY
    zz, yy = sp // NY, lax.rem(sp, NY)
    length, depth = tok.shape
    half = length // 2
    tau = NS * length // 16
    LK = GLA_KEY
    RP = LK // NZ
    groups = (W1, W2)

    def at_z(d):
        return {"sp": lax.rem(zz + d, NZ) * NY + yy}

    def at_y(d):
        return {"sp": zz * NY + lax.rem(yy + d, NY)}

    def at_f(d):
        return {"fs": lax.rem(f + d, NF)}

    other = {"tp": 1 - t}

    def rc(src, dst, ssem, rsem, dev):
        return pltpu.make_async_remote_copy(
            src_ref=src, dst_ref=dst, send_sem=ssem, recv_sem=rsem, device_id=dev, device_id_type=MESH)

    barrier = pltpu.get_barrier_semaphore()
    greet = [at_z(d) for d in range(1, NZ)] + [at_y(1), at_y(NY - 1)] + [at_f(d) for d in range(1, NF)] + [other]
    for dev in greet:
        pl.semaphore_signal(barrier, inc=1, device_id=dev, device_id_type=MESH)
    own1, own2 = W1.at[zz, yy, t], W2.at[zz, yy, t]
    loads = [
        (tok, toks.at[f]),
        (w_decay, own1.at[:, 0:128]), (w_key, own1.at[:, 128:256]), (w_value, own1.at[:, 256:512]),
        (w_wq, own2.at[:, 0:256]), (w_lq, own2.at[:, 256:384]), (w_gate, own2.at[:, 384:640]),
        (lin_o, out_w.at[0:256]), (win_o, out_w.at[256:512]),
    ]
    local = [pltpu.make_async_copy(a, b, lsem.at[n]) for n, (a, b) in enumerate(loads)]
    for c in local:
        c.start()
    W1[zz, yy, t, :, 512:640] = jnp.concatenate([w_wk[...], w_wv[...]], axis=1)

    i0 = lax.broadcasted_iota(jnp.int32, (length, length), 0)
    s0 = lax.broadcasted_iota(jnp.int32, (length, length), 1)
    for n, h in enumerate(levels):
        ref = (i0 & ~(2 * h - 1)) + h - 1
        later = (i0 & h) != 0
        low = jnp.where(later, ref, i0)
        high = jnp.where(later, i0, ref)
        sums[n] = jnp.where((s0 > low) & (s0 <= high), 1.0, 0.0).astype(bf16)
    sums[len(levels)] = jnp.where(s0 <= i0, 1.0, 0.0).astype(bf16)
    sums[len(levels) + 1] = jnp.where(s0 > i0, 1.0, 0.0).astype(bf16)

    @pl.when(sp == 0)
    def _():
        kvbuf[:, 0:WINDOW, :] = jnp.zeros((NF, WINDOW, kvbuf.shape[2]), bf16)

    for c in local[:7]:
        c.wait()
    pl.semaphore_wait(barrier, len(greet))

    def token_copy(j):
        to_right = j in (0, 2, 4)
        first = j in (0, 3, 4)
        who = f if j < 4 else lax.rem(f + (NF - 1 if to_right else 1), NF)
        ref = toks.at[who, pl.ds(0 if first else half, half)]
        return rc(ref, ref, ts.at[j], tr.at[j], at_f(1 if to_right else NF - 1))

    def slot(g, k, yo):
        return groups[g].at[lax.rem(zz - k + NZ, NZ), lax.rem(yy - yo + NY, NY), t]

    def z_copy(g, d):
        ref = slot(g, 0, 0)
        return rc(ref, ref, zs.at[g, d], zr.at[g, d], at_z(d))

    def y_copy(g, k, side):
        ref = slot(g, k, 0)
        return rc(ref, ref, ys.at[g, side, k], yr.at[g, side, k], at_y(1 if side == 0 else NY - 1))

    def relay_copy(g, k):
        up = k % 2 == 0
        ref = slot(g, k, 1 if up else NY - 1)
        return rc(ref, ref, rs.at[g, k], rr.at[g, k], at_y(1 if up else NY - 1))

    def core_copy(g, k, yo):
        ref = slot(g, k, yo)
        return rc(ref, ref, dsnd.at[g], drcv.at[g], other)

    def core_all(g):
        ref = groups[g].at[:, :, t]
        return rc(ref, ref, dsnd.at[g], drcv.at[g], other)

    zorder = []
    for d in range(1, NZ // 2 + 1):
        zorder += [d] if 2 * d == NZ else [d, NZ - d]

    def pass_y(g, k):
        y_copy(g, k, 0).start()
        y_copy(g, k, 1).start()
        core_copy(g, k, 0).start()

    def z_arrive(g):
        for k in zorder:
            z_copy(g, k).wait_recv()
            pass_y(g, k)

    def y_arrive(g):
        for k in [0] + zorder:
            y_copy(g, k, 0).wait_recv()
            if k % 2 == 0:
                relay_copy(g, k).start()
            core_copy(g, k, 1).start()
            y_copy(g, k, 1).wait_recv()
            if k % 2 == 1:
                relay_copy(g, k).start()
            core_copy(g, k, NY - 1).start()

    def relay_arrive(g):
        for k in [0] + zorder:
            relay_copy(g, k).wait_recv()
            core_copy(g, k, 2).start()

    for d in zorder:
        z_copy(0, d).start()
    for j in range(2):
        token_copy(j).start()
    pass_y(0, 0)
    for j in range(2, 4):
        token_copy(j).start()
    for d in zorder:
        z_copy(1, d).start()
    z_arrive(0)
    token_copy(0).wait_recv()
    token_copy(4).start()
    token_copy(1).wait_recv()
    token_copy(5).start()
    y_arrive(0)
    pass_y(1, 0)
    relay_arrive(0)
    core_all(0).wait_recv()

    def order(i):
        return lax.rem(f + jnp.where(i == 0, 0, jnp.where(i == 1, NF - 1, i - 1)), NF)

    def log_sum(n, b):
        x = dot(sums[n], f2[b])
        return x[:, :LK] + x[:, LK:]

    def halo_copy(b):
        return rc(kvbuf.at[b, pl.ds(length, WINDOW)], kvbuf.at[b, pl.ds(0, WINDOW)], hs.at[b], hr.at[b],
                  {"sp": lax.rem(sp + 1, NS)})

    def piece_copy(b, r, src_sp):
        return rc(lst.at[b, r], arr.at[src_sp], asnd.at[b, r], arcv.at[src_sp], {"sp": r * NY + b})

    lane = lax.broadcasted_iota(jnp.int32, (LK, 128), 1)

    @pl.loop(0, NF)
    def _(i):
        b = order(i)

        @pl.when(i == 1)
        def _():
            z_arrive(1)
            token_copy(2).wait_recv()

        @pl.when(i == 2)
        def _():
            y_arrive(1)
            token_copy(3).wait_recv()

        @pl.when(i == 3)
        def _():
            relay_arrive(1)
            token_copy(4).wait_recv()
            token_copy(5).wait_recv()

        p = dot(toks[b], W1[...].reshape(depth, -1)).astype(bf16)
        x = p[:, :LK].astype(f32) + bias[...]
        forget = (jnp.minimum(x, 0.0) - jnp.log1p(jnp.exp(-jnp.abs(x)))) / tau
        hi = forget.astype(bf16)
        f2[b] = jnp.concatenate([hi, (forget - hi.astype(f32)).astype(bf16)], axis=1)
        k = p[:, LK:2 * LK]
        v = p[:, 2 * LK:2 * LK + GLA_VALUE]
        kkey[b] = k
        val[b] = v
        kvbuf[b, WINDOW:, :] = p[:, 2 * LK + GLA_VALUE:]
        faded = (k.astype(f32) * jnp.exp(log_sum(len(levels) + 1, b))).astype(bf16)
        state = dot_rows(faded, v).astype(bf16)
        total = dot_rows(f2[b], jnp.ones((length, 128), bf16))
        decay = jnp.exp(total[:LK] + total[LK:])
        dhi = decay.astype(bf16)
        dlo = (decay - dhi.astype(f32)).astype(bf16)
        packed = jnp.where(lane < 64, dhi.astype(f32), dlo.astype(f32)).astype(bf16)
        lst[b] = jnp.concatenate([state, packed], axis=1).reshape(NZ, RP, GLA_VALUE + 128)

        @pl.when(sp < NS - 1)
        def _():
            halo_copy(b).start()

        @pl.loop(0, NZ)
        def _(r):
            @pl.when(r * NY + b != sp)
            def _():
                piece_copy(b, r, sp).start()

            @pl.when(r * NY + b == sp)
            def _():
                arr[sp] = lst[b, r]

    core_all(1).wait_recv()

    def prefix_copy(s):
        return rc(pre.at[s], state_in.at[yy, zz], qs.at[s], qr.at[sp], {"sp": s})

    def scan():
        def step(s, carry):
            @pl.when(s != sp)
            def _():
                piece_copy(0, 0, s).wait_recv()

            pre[s] = carry.astype(bf16)
            x = arr[s].astype(f32)
            g = x[:, GLA_VALUE:]
            g = g + pltpu.roll(g, 64, 1)
            return carry * jnp.concatenate([g, g], axis=1) + x[:, :GLA_VALUE]

        lax.fori_loop(0, NS, step, jnp.zeros((RP, GLA_VALUE), f32))

        @pl.loop(0, NS)
        def _(s):
            @pl.when(s != sp)
            def _():
                prefix_copy(s).start()

            @pl.when(s == sp)
            def _():
                state_in[yy, zz] = pre[s]

    span = length + WINDOW
    row = lax.broadcasted_iota(jnp.int32, (length, span), 0)
    col = lax.broadcasted_iota(jnp.int32, (length, span), 1)
    distance = row - col + WINDOW
    heads = sink.shape[1]
    wq = heads * HEAD_DIM

    @pl.loop(0, NF)
    def _(i):
        b = order(i)

        @pl.when(i == 2)
        def _():
            scan()

        @pl.when(sp > 0)
        def _():
            halo_copy(b).wait_recv()

        p = dot(toks[b], W2[...].reshape(depth, -1)).astype(bf16)
        allowed = (distance >= 0) & (distance < WINDOW) & ((col >= WINDOW) | (sp > 0))
        kv = kvbuf[b]
        k, v = kv[:, :HEAD_DIM], kv[:, HEAD_DIM:]
        heads_out = []
        for j in range(heads):
            score = dot_t(p[:, j * HEAD_DIM:(j + 1) * HEAD_DIM], k) * HEAD_DIM ** -0.5
            score = jnp.where(allowed, score, -jnp.inf)
            sk = sink[0:1, j:j + 1]
            top = jnp.maximum(jnp.max(score, axis=1, keepdims=True), sk)
            e = jnp.exp(score - top)
            total = jnp.sum(e, axis=1, keepdims=True) + jnp.exp(sk - top)
            heads_out.append((dot(e.astype(bf16), v) / total).astype(bf16))
        rows[b, :, GLA_VALUE:] = jnp.concatenate(heads_out, axis=1)
        gates[b] = p[:, wq + LK:]
        q = p[:, wq:wq + LK].astype(f32) * LK ** -0.5
        k = kkey[b].astype(f32)
        ri = lax.broadcasted_iota(jnp.int32, (length, length), 0)
        ci = lax.broadcasted_iota(jnp.int32, (length, length), 1)
        rk = lax.broadcasted_iota(jnp.int32, (length, LK), 0)
        scores = jnp.where(ri == ci, dot_t(q.astype(bf16), kkey[b]), 0.0)
        for n, h in enumerate(levels):
            decay = jnp.exp(log_sum(n, b))
            later = (rk & h) != 0
            qh = jnp.where(later, q * decay, 0.0).astype(bf16)
            kh = jnp.where(later, 0.0, k * decay).astype(bf16)
            same = (ri & ~(2 * h - 1)) == (ci & ~(2 * h - 1))
            scores = scores + jnp.where(same, dot_t(qh, kh), 0.0)
        reach[b] = (q * jnp.exp(log_sum(len(levels), b))).astype(bf16)
        oacc[b] = dot(scores.astype(bf16), val[b])

    for c in local[7:]:
        c.wait()

    def part_copy(d):
        return rc(part.at[d], rbuf.at[d], ps.at[d], pr.at[d], at_f(d))

    @pl.loop(1, NF + 1)
    def _(step):
        b = lax.rem(f + step, NF)

        @pl.loop(0, NZ)
        def _(r):
            o = r * NY + b

            @pl.when(o != sp)
            def _():
                rc(pre.at[0], state_in.at[b, r], qs.at[0], qr.at[o], {"sp": o}).wait_recv()

        gate = gates[b].astype(f32)
        o = oacc[b] + dot(reach[b], state_in[b].reshape(LK, GLA_VALUE))
        scaled = o * lax.rsqrt(jnp.mean(o * o, axis=1, keepdims=True) + norm_epsilon)
        rows[b, :, :GLA_VALUE] = (scaled * gain[...] * (gate / (1.0 + jnp.exp(-gate)))).astype(bf16)
        y = dot(rows[b], out_w[...])

        @pl.when(step < NF)
        def _():
            part[step] = y.astype(bf16)
            part_copy(step).start()

        @pl.when(step == NF)
        def _():
            acc = y
            for d in range(1, NF):
                part_copy(d).wait_recv()
                acc = acc + rbuf[d].astype(f32)
            out[...] = acc.astype(bf16)

    for j in range(6):
        token_copy(j).wait_send()
    for d in range(1, NF):
        part_copy(d).wait_send()
    for g in range(2):
        for d in range(1, NZ):
            z_copy(g, d).wait_send()
        for k in range(NZ):
            y_copy(g, k, 0).wait_send()
            y_copy(g, k, 1).wait_send()
            relay_copy(g, k).wait_send()
        core_all(g).wait_send()

    @pl.when(sp < NS - 1)
    def _():
        for b in range(NF):
            halo_copy(b).wait_send()

    @pl.loop(0, NS)
    def _(s):
        @pl.when(s != sp)
        def _():
            piece_copy(lax.rem(s, NY), s // NY, sp).wait_send()
            prefix_copy(s).wait_send()


def shards(
    NS, NF, NT,
    tokens, linear_query, linear_key, linear_decay, linear_value, linear_gate, decay_bias,
    norm_gain, window_query, window_key, window_value, sink_logit, linear_output, window_output,
):
    _, length, depth = tokens.shape
    kb = linear_query.shape[0]
    NZ = NS // NY
    levels = []
    h = 1
    while h < length:
        levels.append(h)
        h *= 2
    vm = pltpu.VMEM
    dma = pltpu.SemaphoreType.DMA
    kv_width = window_key.shape[1] + window_value.shape[1]
    out_rows = linear_output.shape[0] + window_output.shape[0]
    width1 = 2 * GLA_KEY + GLA_VALUE + kv_width
    width2 = window_query.shape[1] + GLA_KEY + GLA_VALUE
    anyspec = pl.BlockSpec(memory_space=pl.ANY)
    vspec = pl.BlockSpec(memory_space=vm)
    result = pl.pallas_call(
        functools.partial(kernel, NS, NF, NT, tuple(levels)),
        out_shape=jax.ShapeDtypeStruct((length, depth), bf16),
        in_specs=[anyspec] * 9 + [vspec] * 5,
        out_specs=vspec,
        scratch_shapes=[
            vm((NF, length, depth), bf16),
            vm((NZ, NY, NT, kb, width1), bf16),
            vm((NZ, NY, NT, kb, width2), bf16),
            vm((out_rows, depth), bf16),
            vm((len(levels) + 2, length, length), bf16),
            vm((NF, length, 2 * GLA_KEY), bf16),
            vm((NF, length, GLA_KEY), bf16),
            vm((NF, length, GLA_VALUE), bf16),
            vm((NF, length + WINDOW, kv_width), bf16),
            vm((NF, NZ, GLA_KEY // NZ, GLA_VALUE + 128), bf16),
            vm((NS, GLA_KEY // NZ, GLA_VALUE + 128), bf16),
            vm((NS, GLA_KEY // NZ, GLA_VALUE), bf16),
            vm((NF, NZ, GLA_KEY // NZ, GLA_VALUE), bf16),
            vm((NF, length, out_rows), bf16),
            vm((NF, length, GLA_VALUE), f32),
            vm((NF, length, GLA_KEY), bf16),
            vm((NF, length, GLA_VALUE), bf16),
            vm((NF, length, depth), bf16),
            vm((NF, length, depth), bf16),
            dma((9,)),
            dma((2, NZ)), dma((2, NZ)),
            dma((2, 2, NZ)), dma((2, 2, NZ)),
            dma((2, NZ)), dma((2, NZ)),
            dma((2,)), dma((2,)),
            dma((6,)), dma((6,)),
            dma((NF,)), dma((NF,)),
            dma((NF, NZ)), dma((NS,)),
            dma((NS,)), dma((NS,)),
            dma((NF,)), dma((NF,)),
        ],
        compiler_params=pltpu.CompilerParams(
            collective_id=0, has_side_effects=True, vmem_limit_bytes=60 * 1024 * 1024),
        name="layer",
    )(tokens[0], linear_decay, linear_key, linear_value, window_query, linear_query, linear_gate,
      linear_output, window_output, window_key, window_value,
      decay_bias[None], norm_gain[None], sink_logit[None])
    return result[None]


def solution(mesh):
    shape = mesh.shape
    return jax.shard_map(
        functools.partial(shards, shape["sp"], shape["fs"], shape["tp"]),
        mesh=mesh,
        in_specs=(
            P(("fs", "tp"), "sp", None),
            P(("sp", "tp"), "fs"),
            P(("sp", "tp"), "fs"),
            P(("sp", "tp"), "fs"),
            P(("sp", "tp"), "fs"),
            P(("sp", "tp"), "fs"),
            P("fs"),
            P(),
            P(("sp", "tp"), "fs"),
            P(("sp", "tp"), "fs"),
            P(("sp", "tp"), "fs"),
            P("fs"),
            P("fs", None),
            P("fs", None),
        ),
        out_specs=P(("fs", "tp"), "sp", None),
        check_vma=False,
    )
```

```python
import functools

import jax
import jax.numpy as jnp
from jax import lax
from jax.experimental import pallas as pl
from jax.experimental.pallas import tpu as pltpu
from jax.sharding import PartitionSpec as P

GLA_KEY = 128
GLA_VALUE = 256
HEAD_DIM = 64
WINDOW = 128
NY = 4

norm_epsilon = 1e-05
MESH = pl.DeviceIdType.MESH
f32, bf16 = jnp.float32, jnp.bfloat16


def dot(a, b):
    return jnp.dot(a, b, preferred_element_type=f32)


def dot_t(a, b):
    return lax.dot_general(a, b, (((1,), (1,)), ((), ())), preferred_element_type=f32)


def dot_rows(a, b):
    return lax.dot_general(a, b, (((0,), (0,)), ((), ())), preferred_element_type=f32)


def kernel(
    NS, NF, NT, levels,
    tok, w_decay, w_key, w_value, w_lq, w_wq, w_gate, lin_o, win_o, w_wk, w_wv, bias, gain, sink,
    out,
    toks, W1, W2, OW, sums, f2, kkey, val, query, kvbuf, lst, arr, pre, state_in,
    lrow, wrow, lall, wall, oacc, reach, gates, acc,
    lsem, zs, zr, ys, yr, rs, rr, dsnd, drcv, ts, tr, hs, hr, asnd, arcv, qs, qr,
    ls, lr, ws, wr, xs, xr, os, orr,
):
    sp, f, t = lax.axis_index("sp"), lax.axis_index("fs"), lax.axis_index("tp")
    NZ = NS // NY
    zz, yy = sp // NY, lax.rem(sp, NY)
    length, depth = tok.shape
    half = length // 2
    tau = NS * length // 16
    LK = GLA_KEY
    RP = LK // NZ
    groups = (W1, W2)
    scope = jax.named_scope

    def at_z(d):
        return {"sp": lax.rem(zz + d, NZ) * NY + yy}

    def at_y(d):
        return {"sp": zz * NY + lax.rem(yy + d, NY)}

    def at_f(d):
        return {"fs": lax.rem(f + d, NF)}

    other = {"tp": 1 - t}

    def rc(src, dst, ssem, rsem, dev):
        return pltpu.make_async_remote_copy(
            src_ref=src, dst_ref=dst, send_sem=ssem, recv_sem=rsem, device_id=dev, device_id_type=MESH)

    barrier = pltpu.get_barrier_semaphore()
    greet = [at_z(d) for d in range(1, NZ)] + [at_y(1), at_y(NY - 1)] + [at_f(d) for d in range(1, NF)] + [other]
    for dev in greet:
        pl.semaphore_signal(barrier, inc=1, device_id=dev, device_id_type=MESH)
    own1, own2 = W1.at[zz, yy, t], W2.at[zz, yy, t]
    loads = [
        (tok, toks.at[f]),
        (w_decay, own1.at[:, 0:128]), (w_key, own1.at[:, 128:256]), (w_value, own1.at[:, 256:512]),
        (w_lq, own1.at[:, 512:640]),
        (w_wq, own2.at[:, 0:256]), (w_gate, own2.at[:, 256:512]),
        (lin_o, OW.at[0]), (win_o, OW.at[NF]),
    ]
    local = [pltpu.make_async_copy(a, b, lsem.at[n]) for n, (a, b) in enumerate(loads)]
    for c in local:
        c.start()
    W1[zz, yy, t, :, 640:768] = jnp.concatenate([w_wk[...], w_wv[...]], axis=1)

    i0 = lax.broadcasted_iota(jnp.int32, (length, length), 0)
    s0 = lax.broadcasted_iota(jnp.int32, (length, length), 1)
    for n, h in enumerate(levels):
        ref = (i0 & ~(2 * h - 1)) + h - 1
        later = (i0 & h) != 0
        low = jnp.where(later, ref, i0)
        high = jnp.where(later, i0, ref)
        sums[n] = jnp.where((s0 > low) & (s0 <= high), 1.0, 0.0).astype(bf16)
    sums[len(levels)] = jnp.where(s0 <= i0, 1.0, 0.0).astype(bf16)
    sums[len(levels) + 1] = jnp.where(s0 > i0, 1.0, 0.0).astype(bf16)

    @pl.when(sp == 0)
    def _():
        kvbuf[:, 0:WINDOW, :] = jnp.zeros((NF, WINDOW, kvbuf.shape[2]), bf16)

    with scope("a_loads"):
        for c in local[:7]:
            c.wait()
    with scope("b_barrier"):
        pl.semaphore_wait(barrier, len(greet))

    def x_step(j):
        return j in (0, 2, 4), j in (0, 3, 4)

    def token_copy(j):
        right, first = x_step(j)
        who = f if j < 4 else lax.rem(f + (NF - 1 if right else 1), NF)
        ref = toks.at[who, pl.ds(0 if first else half, half)]
        return rc(ref, ref, ts.at[j], tr.at[j], at_f(1 if right else NF - 1))

    orows = OW.shape[1]
    ocols = depth // NT
    cols_t = pl.ds(pl.multiple_of(t * ocols, ocols), ocols)

    def ow_part(rel, first):
        return OW.at[NF + rel, pl.ds(0 if first else orows // 2, orows // 2), cols_t]

    def ow_copy(j):
        right, first = x_step(j)
        src = 0 if j < 4 else (NF - 1 if right else 1)
        dst = (src + (NF - 1 if right else 1)) % NF
        return rc(ow_part(src, first), ow_part(dst, first), os.at[j], orr.at[j], at_f(1 if right else NF - 1))

    def ow_core(j):
        right, first = x_step(j)
        ref = ow_part((NF - 1 if right else 1) if j < 4 else 2, first)
        return rc(ref, ref, dsnd.at[3], drcv.at[3], other)

    def ow_core_all():
        ref = OW.at[pl.ds(NF + 1, NF - 1), :, cols_t]
        return rc(ref, ref, dsnd.at[3], drcv.at[3], other)

    tile_r = orows // (NS // 2)
    tile_c = ocols // 2

    def ow_tile(k, yo):
        z1, y1 = lax.rem(zz - k + NZ, NZ), lax.rem(yy - yo + NY, NY)
        s1 = z1 * NY + y1
        return (pl.ds(pl.multiple_of((s1 // 2) * tile_r, tile_r), tile_r),
                pl.ds(pl.multiple_of((t * 2 + lax.rem(s1, 2)) * tile_c, tile_c), tile_c))

    def slice_copy(d):
        r, c = ow_tile(0, 0)
        return rc(OW.at[0, r, c], OW.at[NF - d, r, c], xs.at[d], xr.at[d], at_f(d))

    def slot(g, k, yo):
        if g == 2:
            r, c = ow_tile(k, yo)
            return OW.at[pl.ds(1, NF - 1), r, c]
        return groups[g].at[lax.rem(zz - k + NZ, NZ), lax.rem(yy - yo + NY, NY), t]

    def z_copy(g, d):
        ref = slot(g, 0, 0)
        return rc(ref, ref, zs.at[g, d], zr.at[g, d], at_z(d))

    def y_copy(g, k, side):
        ref = slot(g, k, 0)
        return rc(ref, ref, ys.at[g, side, k], yr.at[g, side, k], at_y(1 if side == 0 else NY - 1))

    def relay_copy(g, k):
        up = k % 2 == 0
        ref = slot(g, k, 1 if up else NY - 1)
        return rc(ref, ref, rs.at[g, k], rr.at[g, k], at_y(1 if up else NY - 1))

    def core_copy(g, k, yo):
        ref = slot(g, k, yo)
        return rc(ref, ref, dsnd.at[g], drcv.at[g], other)

    def core_all(g):
        ref = OW.at[pl.ds(1, NF - 1), :, cols_t] if g == 2 else groups[g].at[:, :, t]
        return rc(ref, ref, dsnd.at[g], drcv.at[g], other)

    zorder = []
    for d in range(1, NZ // 2 + 1):
        zorder += [d] if 2 * d == NZ else [d, NZ - d]

    def z_send(g):
        for d in zorder:
            z_copy(g, d).start()

    def pass_y(g, k):
        y_copy(g, k, 0).start()
        y_copy(g, k, 1).start()
        core_copy(g, k, 0).start()

    def z_arrive(g):
        for k in zorder:
            z_copy(g, k).wait_recv()
            pass_y(g, k)

    def y_arrive(g):
        for k in [0] + zorder:
            y_copy(g, k, 0).wait_recv()
            if k % 2 == 0:
                relay_copy(g, k).start()
            core_copy(g, k, 1).start()
            y_copy(g, k, 1).wait_recv()
            if k % 2 == 1:
                relay_copy(g, k).start()
            core_copy(g, k, NY - 1).start()

    def relay_arrive(g):
        for k in [0] + zorder:
            relay_copy(g, k).wait_recv()
            core_copy(g, k, 2).start()

    z_send(0)
    for j in range(2):
        token_copy(j).start()
    pass_y(0, 0)
    for j in range(2, 4):
        token_copy(j).start()
    z_send(1)
    with scope("c_z0"):
        z_arrive(0)
    with scope("d_tokfwd"):
        for j in range(2):
            token_copy(j).wait_recv()
            token_copy(4 + j).start()
    for c in local[7:]:
        c.wait()
    for d in range(1, NF):
        slice_copy(d).start()
    for j in range(4):
        ow_copy(j).start()
    with scope("e_y0"):
        y_arrive(0)
    pass_y(1, 0)
    with scope("e_z1"):
        z_arrive(1)
    with scope("f_relay0"):
        relay_arrive(0)
    with scope("g_core0"):
        core_all(0).wait_recv()

    def order(i):
        return lax.rem(f + jnp.where(i == 0, 0, jnp.where(i == 1, NF - 1, i - 1)), NF)

    def log_sum(n, b):
        x = dot(sums[n], f2[b])
        return x[:, :LK] + x[:, LK:]

    def halo_copy(b):
        return rc(kvbuf.at[b, pl.ds(length, WINDOW)], kvbuf.at[b, pl.ds(0, WINDOW)], hs.at[b], hr.at[b],
                  {"sp": lax.rem(sp + 1, NS)})

    def piece_copy(b, r, src_sp):
        return rc(lst.at[b, r], arr.at[src_sp], asnd.at[b, r], arcv.at[src_sp], {"sp": r * NY + b})

    lane = lax.broadcasted_iota(jnp.int32, (LK, 128), 1)

    @pl.loop(0, NF)
    def _(i):
        b = order(i)

        @pl.when(i == 1)
        def _():
            with scope("h_tok1"):
                token_copy(2).wait_recv()

        @pl.when(i == 2)
        def _():
            with scope("h_tok2"):
                token_copy(3).wait_recv()

        @pl.when(i == 3)
        def _():
            with scope("h_tok3"):
                token_copy(4).wait_recv()
                token_copy(5).wait_recv()

        p = dot(toks[b], W1[...].reshape(depth, -1)).astype(bf16)
        x = p[:, :LK].astype(f32) + bias[...]
        forget = (jnp.minimum(x, 0.0) - jnp.log1p(jnp.exp(-jnp.abs(x)))) / tau
        hi = forget.astype(bf16)
        f2[b] = jnp.concatenate([hi, (forget - hi.astype(f32)).astype(bf16)], axis=1)
        k = p[:, LK:2 * LK]
        v = p[:, 2 * LK:2 * LK + GLA_VALUE]
        kkey[b] = k
        val[b] = v
        query[b] = p[:, 512:640]
        kvbuf[b, WINDOW:, :] = p[:, 640:]
        faded = (k.astype(f32) * jnp.exp(log_sum(len(levels) + 1, b))).astype(bf16)
        state = dot_rows(faded, v).astype(bf16)
        total = dot_rows(f2[b], jnp.ones((length, 128), bf16))
        decay = jnp.exp(total[:LK] + total[LK:])
        dhi = decay.astype(bf16)
        dlo = (decay - dhi.astype(f32)).astype(bf16)
        packed = jnp.where(lane < 64, dhi.astype(f32), dlo.astype(f32)).astype(bf16)
        lst[b] = jnp.concatenate([state, packed], axis=1).reshape(NZ, RP, GLA_VALUE + 128)

        @pl.loop(0, NZ)
        def _(r):
            @pl.when(r * NY + b != sp)
            def _():
                piece_copy(b, r, sp).start()

            @pl.when(r * NY + b == sp)
            def _():
                arr[sp] = lst[b, r]

        @pl.when(sp < NS - 1)
        def _():
            halo_copy(b).start()

    with scope("i_y1"):
        y_arrive(1)

    @pl.loop(0, NF)
    def _(i):
        b = order(i)

        @pl.when(i == 1)
        def _():
            with scope("i_xs"):
                for d in range(1, NF):
                    slice_copy(d).wait_recv()
                z_send(2)
                pass_y(2, 0)

        @pl.when(i == 2)
        def _():
            with scope("i_relay1"):
                relay_arrive(1)

        @pl.when(i == 3)
        def _():
            with scope("i_owx"):
                for j in range(2):
                    ow_copy(j).wait_recv()
                    ow_copy(4 + j).start()
                    ow_core(j).start()

        q = query[b].astype(f32) * LK ** -0.5
        k = kkey[b].astype(f32)
        ri = lax.broadcasted_iota(jnp.int32, (length, length), 0)
        ci = lax.broadcasted_iota(jnp.int32, (length, length), 1)
        rk = lax.broadcasted_iota(jnp.int32, (length, LK), 0)
        scores = jnp.where(ri == ci, dot_t(q.astype(bf16), kkey[b]), 0.0)
        for n, h in enumerate(levels):
            decay = jnp.exp(log_sum(n, b))
            later = (rk & h) != 0
            qh = jnp.where(later, q * decay, 0.0).astype(bf16)
            kh = jnp.where(later, 0.0, k * decay).astype(bf16)
            same = (ri & ~(2 * h - 1)) == (ci & ~(2 * h - 1))
            scores = scores + jnp.where(same, dot_t(qh, kh), 0.0)
        reach[b] = (q * jnp.exp(log_sum(len(levels), b))).astype(bf16)
        oacc[b] = dot(scores.astype(bf16), val[b])

    with scope("k_core1"):
        core_all(1).wait_recv()

    def prefix_copy(s):
        return rc(pre.at[s], state_in.at[yy, zz], qs.at[s], qr.at[sp], {"sp": s})

    def scan():
        def step(s, carry):
            @pl.when(s != sp)
            def _():
                piece_copy(0, 0, s).wait_recv()

            pre[s] = carry.astype(bf16)
            x = arr[s].astype(f32)
            g = x[:, GLA_VALUE:]
            g = g + pltpu.roll(g, 64, 1)
            return carry * jnp.concatenate([g, g], axis=1) + x[:, :GLA_VALUE]

        with scope("l_scan"):
            lax.fori_loop(0, NS, step, jnp.zeros((RP, GLA_VALUE), f32))

        @pl.loop(0, NS)
        def _(s):
            @pl.when(s != sp)
            def _():
                prefix_copy(s).start()

            @pl.when(s == sp)
            def _():
                state_in[yy, zz] = pre[s]

    span = length + WINDOW
    row = lax.broadcasted_iota(jnp.int32, (length, span), 0)
    col = lax.broadcasted_iota(jnp.int32, (length, span), 1)
    distance = row - col + WINDOW
    heads = sink.shape[1]
    wq = heads * HEAD_DIM

    def rows_copy(src, dst, ssem, rsem, off):
        return rc(src.at[off], dst.at[lax.rem(NF - off, NF)], ssem.at[off], rsem.at[off], at_f(off))

    def wrow_copy(off):
        return rows_copy(wrow, wall, ws, wr, off)

    def lrow_copy(off):
        return rows_copy(lrow, lall, ls, lr, off)

    @pl.loop(0, NF)
    def _(i):
        b = order(i)
        off = lax.rem(b - f + NF, NF)

        @pl.when(i == 0)
        def _():
            scan()

        @pl.when(i == 1)
        def _():
            with scope("m_z2"):
                z_arrive(2)

        @pl.when(i == 2)
        def _():
            with scope("m_owx2"):
                for j in range(2, 4):
                    ow_copy(j).wait_recv()
                    ow_core(j).start()

        @pl.when(i == 3)
        def _():
            with scope("m_y2"):
                y_arrive(2)

        @pl.when(sp > 0)
        def _():
            halo_copy(b).wait_recv()

        p = dot(toks[b], W2[...].reshape(depth, -1)).astype(bf16)
        allowed = (distance >= 0) & (distance < WINDOW) & ((col >= WINDOW) | (sp > 0))
        kv = kvbuf[b]
        k, v = kv[:, :HEAD_DIM], kv[:, HEAD_DIM:]
        heads_out = []
        for j in range(heads):
            score = dot_t(p[:, j * HEAD_DIM:(j + 1) * HEAD_DIM], k) * HEAD_DIM ** -0.5
            score = jnp.where(allowed, score, -jnp.inf)
            sk = sink[0:1, j:j + 1]
            top = jnp.maximum(jnp.max(score, axis=1, keepdims=True), sk)
            e = jnp.exp(score - top)
            total = jnp.sum(e, axis=1, keepdims=True) + jnp.exp(sk - top)
            heads_out.append((dot(e.astype(bf16), v) / total).astype(bf16))
        gates[b] = p[:, wq:]
        win = jnp.concatenate(heads_out, axis=1)

        @pl.when(i == 0)
        def _():
            wall[0] = win

        @pl.when(i > 0)
        def _():
            wrow[off] = win
            wrow_copy(off).start()

    @pl.loop(0, NF)
    def _(i):
        off = jnp.where(i == 0, 2, jnp.where(i == 1, NF - 1, jnp.where(i == 2, 1, 0)))
        b = lax.rem(f + off, NF)

        with scope("o_state"):
            @pl.loop(0, NZ)
            def _(r):
                o = r * NY + b

                @pl.when(o != sp)
                def _():
                    rc(pre.at[0], state_in.at[b, r], qs.at[0], qr.at[o], {"sp": o}).wait_recv()

        gate = gates[b].astype(f32)
        o = oacc[b] + dot(reach[b], state_in[b].reshape(LK, GLA_VALUE))
        scaled = o * lax.rsqrt(jnp.mean(o * o, axis=1, keepdims=True) + norm_epsilon)
        lin = (scaled * gain[...] * (gate / (1.0 + jnp.exp(-gate)))).astype(bf16)

        @pl.when(off == 0)
        def _():
            lall[0] = lin

        @pl.when(off > 0)
        def _():
            lrow[off] = lin
            lrow_copy(off).start()

    with scope("p_ow"):
        relay_arrive(2)
        for j in range(4, 6):
            ow_copy(j).wait_recv()
            ow_core(j).start()
        ow_core_all().wait_recv()
    with scope("p_wrow"):
        for off in range(1, NF):
            wrow_copy(off).wait_recv()

    chunk = 512

    def project(kind, rows_of, init):
        left = jnp.concatenate([rows_of[n] for n in range(NF)], axis=1)
        for c in range(depth // chunk):
            cs = slice(c * chunk, (c + 1) * chunk)
            y = dot(left, OW[kind * NF:(kind + 1) * NF, :, cs].reshape(NF * orows, chunk))
            if init:
                acc[:, cs] = y
            else:
                out[:, cs] = (acc[:, cs] + y).astype(bf16)

    with scope("q_proj1"):
        project(1, wall, True)
    with scope("r_core2"):
        core_all(2).wait_recv()
    with scope("r_lrow"):
        for off in range(1, NF):
            lrow_copy(off).wait_recv()
    with scope("s_proj2"):
        project(0, lall, False)

    with scope("t_end"):
        for j in range(6):
            token_copy(j).wait_send()
            ow_copy(j).wait_send()
        for d in range(1, NF):
            slice_copy(d).wait_send()
            wrow_copy(d).wait_send()
            lrow_copy(d).wait_send()
        for g in range(3):
            for d in range(1, NZ):
                z_copy(g, d).wait_send()
            for k in range(NZ):
                y_copy(g, k, 0).wait_send()
                y_copy(g, k, 1).wait_send()
                relay_copy(g, k).wait_send()
            core_all(g).wait_send()
        ow_core_all().wait_send()

        @pl.when(sp < NS - 1)
        def _():
            for b in range(NF):
                halo_copy(b).wait_send()

        @pl.loop(0, NS)
        def _(s):
            @pl.when(s != sp)
            def _():
                piece_copy(lax.rem(s, NY), s // NY, sp).wait_send()
                prefix_copy(s).wait_send()


def shards(
    NS, NF, NT,
    tokens, linear_query, linear_key, linear_decay, linear_value, linear_gate, decay_bias,
    norm_gain, window_query, window_key, window_value, sink_logit, linear_output, window_output,
):
    _, length, depth = tokens.shape
    kb = linear_query.shape[0]
    NZ = NS // NY
    levels = []
    h = 1
    while h < length:
        levels.append(h)
        h *= 2
    vm = pltpu.VMEM
    dma = pltpu.SemaphoreType.DMA
    kv_width = window_key.shape[1] + window_value.shape[1]
    width1 = 3 * GLA_KEY + GLA_VALUE + kv_width
    width2 = window_query.shape[1] + GLA_VALUE
    anyspec = pl.BlockSpec(memory_space=pl.ANY)
    vspec = pl.BlockSpec(memory_space=vm)
    result = pl.pallas_call(
        functools.partial(kernel, NS, NF, NT, tuple(levels)),
        out_shape=jax.ShapeDtypeStruct((length, depth), bf16),
        in_specs=[anyspec] * 9 + [vspec] * 5,
        out_specs=vspec,
        scratch_shapes=[
            vm((NF, length, depth), bf16),
            vm((NZ, NY, NT, kb, width1), bf16),
            vm((NZ, NY, NT, kb, width2), bf16),
            vm((2 * NF, linear_output.shape[0], depth), bf16),
            vm((len(levels) + 2, length, length), bf16),
            vm((NF, length, 2 * GLA_KEY), bf16),
            vm((NF, length, GLA_KEY), bf16),
            vm((NF, length, GLA_VALUE), bf16),
            vm((NF, length, GLA_KEY), bf16),
            vm((NF, length + WINDOW, kv_width), bf16),
            vm((NF, NZ, GLA_KEY // NZ, GLA_VALUE + 128), bf16),
            vm((NS, GLA_KEY // NZ, GLA_VALUE + 128), bf16),
            vm((NS, GLA_KEY // NZ, GLA_VALUE), bf16),
            vm((NF, NZ, GLA_KEY // NZ, GLA_VALUE), bf16),
            vm((NF, length, GLA_VALUE), bf16),
            vm((NF, length, window_query.shape[1]), bf16),
            vm((NF, length, GLA_VALUE), bf16),
            vm((NF, length, window_query.shape[1]), bf16),
            vm((NF, length, GLA_VALUE), f32),
            vm((NF, length, GLA_KEY), bf16),
            vm((NF, length, GLA_VALUE), bf16),
            vm((length, depth), f32),
            dma((9,)),
            dma((3, NZ)), dma((3, NZ)),
            dma((3, 2, NZ)), dma((3, 2, NZ)),
            dma((3, NZ)), dma((3, NZ)),
            dma((4,)), dma((4,)),
            dma((6,)), dma((6,)),
            dma((NF,)), dma((NF,)),
            dma((NF, NZ)), dma((NS,)),
            dma((NS,)), dma((NS,)),
            dma((NF,)), dma((NF,)),
            dma((NF,)), dma((NF,)),
            dma((NF,)), dma((NF,)),
            dma((6,)), dma((6,)),
        ],
        compiler_params=pltpu.CompilerParams(
            collective_id=0, has_side_effects=True, vmem_limit_bytes=60 * 1024 * 1024),
        name="layer",
    )(tokens[0], linear_decay, linear_key, linear_value, linear_query, window_query, linear_gate,
      linear_output, window_output, window_key, window_value,
      decay_bias[None], norm_gain[None], sink_logit[None])
    return result[None]


def solution(mesh):
    shape = mesh.shape
    return jax.shard_map(
        functools.partial(shards, shape["sp"], shape["fs"], shape["tp"]),
        mesh=mesh,
        in_specs=(
            P(("fs", "tp"), "sp", None),
            P(("sp", "tp"), "fs"),
            P(("sp", "tp"), "fs"),
            P(("sp", "tp"), "fs"),
            P(("sp", "tp"), "fs"),
            P(("sp", "tp"), "fs"),
            P("fs"),
            P(),
            P(("sp", "tp"), "fs"),
            P(("sp", "tp"), "fs"),
            P(("sp", "tp"), "fs"),
            P("fs"),
            P("fs", None),
            P("fs", None),
        ),
        out_specs=P(("fs", "tp"), "sp", None),
        check_vma=False,
    )
```

```python
import functools

import jax
import jax.numpy as jnp
from jax import lax
from jax.experimental import pallas as pl
from jax.experimental.pallas import tpu as pltpu
from jax.sharding import PartitionSpec as P

GLA_KEY = 128
GLA_VALUE = 256
HEAD_DIM = 64
WINDOW = 128
NY = 4

norm_epsilon = 1e-05
MESH = pl.DeviceIdType.MESH
f32, bf16 = jnp.float32, jnp.bfloat16


def dot(a, b):
    return jnp.dot(a, b, preferred_element_type=f32)


def dot_t(a, b):
    return lax.dot_general(a, b, (((1,), (1,)), ((), ())), preferred_element_type=f32)


def dot_rows(a, b):
    return lax.dot_general(a, b, (((0,), (0,)), ((), ())), preferred_element_type=f32)


def kernel(
    NS, NF, NT, levels,
    tok, w_decay, w_key, w_value, w_lq, w_wq, w_gate, lin_o, win_o, w_wk, w_wv, bias, gain, sink,
    out,
    toks, W1, W2, OW, sums, f2, kkey, val, query, kvbuf, lst, arr, pre, state_in,
    lrow, wrow, lall, wall, oacc, reach, gates, acc,
    obuf, lsem, zs, zr, ys, yr, rs, rr, dsnd, drcv, ts, tr, hs, hr, asnd, arcv, qs, qr,
    ls, lr, ws, wr, xs, xr, os, orr,
):
    sp, f, t = lax.axis_index("sp"), lax.axis_index("fs"), lax.axis_index("tp")
    NZ = NS // NY
    zz, yy = sp // NY, lax.rem(sp, NY)
    length, depth = tok.shape
    half = length // 2
    tau = NS * length // 16
    LK = GLA_KEY
    RP = LK // NZ
    groups = (W1, W2)
    scope = jax.named_scope

    def at_z(d):
        return {"sp": lax.rem(zz + d, NZ) * NY + yy}

    def at_y(d):
        return {"sp": zz * NY + lax.rem(yy + d, NY)}

    def at_f(d):
        return {"fs": lax.rem(f + d, NF)}

    other = {"tp": 1 - t}

    def rc(src, dst, ssem, rsem, dev):
        return pltpu.make_async_remote_copy(
            src_ref=src, dst_ref=dst, send_sem=ssem, recv_sem=rsem, device_id=dev, device_id_type=MESH)

    barrier = pltpu.get_barrier_semaphore()
    greet = [at_z(d) for d in range(1, NZ)] + [at_y(1), at_y(NY - 1)] + [at_f(d) for d in range(1, NF)] + [other]
    for dev in greet:
        pl.semaphore_signal(barrier, inc=1, device_id=dev, device_id_type=MESH)
    own1, own2 = W1.at[zz, yy, t], W2.at[zz, yy, t]
    loads = [
        (tok, toks.at[f]),
        (w_decay, own1.at[:, 0:128]), (w_key, own1.at[:, 128:256]), (w_value, own1.at[:, 256:512]),
        (w_lq, own1.at[:, 512:640]),
        (w_wq, own2.at[:, 0:256]), (w_gate, own2.at[:, 256:512]),
        (lin_o, OW.at[0]), (win_o, OW.at[NF]),
    ]
    local = [pltpu.make_async_copy(a, b, lsem.at[n]) for n, (a, b) in enumerate(loads)]
    for c in local:
        c.start()
    W1[zz, yy, t, :, 640:768] = jnp.concatenate([w_wk[...], w_wv[...]], axis=1)

    i0 = lax.broadcasted_iota(jnp.int32, (length, length), 0)
    s0 = lax.broadcasted_iota(jnp.int32, (length, length), 1)
    for n, h in enumerate(levels):
        ref = (i0 & ~(2 * h - 1)) + h - 1
        later = (i0 & h) != 0
        low = jnp.where(later, ref, i0)
        high = jnp.where(later, i0, ref)
        sums[n] = jnp.where((s0 > low) & (s0 <= high), 1.0, 0.0).astype(bf16)
    sums[len(levels)] = jnp.where(s0 <= i0, 1.0, 0.0).astype(bf16)
    sums[len(levels) + 1] = jnp.where(s0 > i0, 1.0, 0.0).astype(bf16)

    @pl.when(sp == 0)
    def _():
        kvbuf[:, 0:WINDOW, :] = jnp.zeros((NF, WINDOW, kvbuf.shape[2]), bf16)

    with scope("a_loads"):
        for c in local[:7]:
            c.wait()
    with scope("b_barrier"):
        pl.semaphore_wait(barrier, len(greet))

    def x_step(j):
        return j in (0, 2, 4), j in (0, 3, 4)

    def token_copy(j):
        right, first = x_step(j)
        who = f if j < 4 else lax.rem(f + (NF - 1 if right else 1), NF)
        ref = toks.at[who, pl.ds(0 if first else half, half)]
        return rc(ref, ref, ts.at[j], tr.at[j], at_f(1 if right else NF - 1))

    orows = OW.shape[1]
    ocols = depth // NT
    cols_t = pl.ds(pl.multiple_of(t * ocols, ocols), ocols)

    def ow_part(rel, first):
        return OW.at[NF + rel, pl.ds(0 if first else orows // 2, orows // 2), cols_t]

    def ow_copy(j):
        right, first = x_step(j)
        src = 0 if j < 4 else (NF - 1 if right else 1)
        dst = (src + (NF - 1 if right else 1)) % NF
        return rc(ow_part(src, first), ow_part(dst, first), os.at[j], orr.at[j], at_f(1 if right else NF - 1))

    def ow_core(j):
        right, first = x_step(j)
        ref = ow_part((NF - 1 if right else 1) if j < 4 else 2, first)
        return rc(ref, ref, dsnd.at[3], drcv.at[3], other)

    def ow_core_all():
        ref = OW.at[pl.ds(NF + 1, NF - 1), :, cols_t]
        return rc(ref, ref, dsnd.at[3], drcv.at[3], other)

    tile_r = orows // (NS // 2)
    tile_c = ocols // 2

    def ow_tile(k, yo):
        z1, y1 = lax.rem(zz - k + NZ, NZ), lax.rem(yy - yo + NY, NY)
        s1 = z1 * NY + y1
        return (pl.ds(pl.multiple_of((s1 // 2) * tile_r, tile_r), tile_r),
                pl.ds(pl.multiple_of((t * 2 + lax.rem(s1, 2)) * tile_c, tile_c), tile_c))

    def slice_copy(d):
        r, c = ow_tile(0, 0)
        return rc(lin_o.at[r, c], OW.at[NF - d, r, c], xs.at[d], xr.at[d], at_f(d))

    def slot(g, k, yo):
        if g == 2:
            r, c = ow_tile(k, yo)
            return OW.at[pl.ds(1, NF - 1), r, c]
        return groups[g].at[lax.rem(zz - k + NZ, NZ), lax.rem(yy - yo + NY, NY), t]

    def z_copy(g, d):
        ref = slot(g, 0, 0)
        return rc(ref, ref, zs.at[g, d], zr.at[g, d], at_z(d))

    def y_copy(g, k, side):
        ref = slot(g, k, 0)
        return rc(ref, ref, ys.at[g, side, k], yr.at[g, side, k], at_y(1 if side == 0 else NY - 1))

    def relay_copy(g, k):
        up = k % 2 == 0
        ref = slot(g, k, 1 if up else NY - 1)
        return rc(ref, ref, rs.at[g, k], rr.at[g, k], at_y(1 if up else NY - 1))

    def core_copy(g, k, yo):
        ref = slot(g, k, yo)
        return rc(ref, ref, dsnd.at[g], drcv.at[g], other)

    def core_all(g):
        ref = OW.at[pl.ds(1, NF - 1), :, cols_t] if g == 2 else groups[g].at[:, :, t]
        return rc(ref, ref, dsnd.at[g], drcv.at[g], other)

    zorder = []
    for d in range(1, NZ // 2 + 1):
        zorder += [d] if 2 * d == NZ else [d, NZ - d]

    def z_send(g):
        for d in zorder:
            z_copy(g, d).start()

    def pass_y(g, k):
        y_copy(g, k, 0).start()
        y_copy(g, k, 1).start()
        core_copy(g, k, 0).start()

    def z_arrive(g, ks=None):
        for k in zorder if ks is None else ks:
            z_copy(g, k).wait_recv()
            pass_y(g, k)

    def y_arrive(g):
        for k in [0] + zorder:
            y_copy(g, k, 0).wait_recv()
            if k % 2 == 0:
                relay_copy(g, k).start()
            core_copy(g, k, 1).start()
            y_copy(g, k, 1).wait_recv()
            if k % 2 == 1:
                relay_copy(g, k).start()
            core_copy(g, k, NY - 1).start()

    def relay_arrive(g):
        for k in [0] + zorder:
            relay_copy(g, k).wait_recv()
            core_copy(g, k, 2).start()

    for d in range(1, NF):
        slice_copy(d).start()
    z_send(0)
    for j in range(2):
        token_copy(j).start()
    pass_y(0, 0)
    for j in range(2, 4):
        token_copy(j).start()
    z_send(1)
    with scope("c_z0"):
        z_arrive(0)
    with scope("d_tokfwd"):
        for j in range(2):
            token_copy(j).wait_recv()
            token_copy(4 + j).start()
    with scope("d_slices"):
        for d in range(1, NF):
            slice_copy(d).wait_recv()
    z_send(2)
    for c in local[7:]:
        c.wait()
    for j in range(4):
        ow_copy(j).start()
    with scope("e_y0"):
        y_arrive(0)
    pass_y(1, 0)
    with scope("e_z1"):
        z_arrive(1)
    with scope("f_relay0"):
        relay_arrive(0)
    pass_y(2, 0)
    with scope("g_core0"):
        core_all(0).wait_recv()

    def order(i):
        return lax.rem(f + jnp.where(i == 0, 0, jnp.where(i == 1, NF - 1, i - 1)), NF)

    def log_sum(n, b):
        x = dot(sums[n], f2[b])
        return x[:, :LK] + x[:, LK:]

    def halo_copy(b):
        return rc(kvbuf.at[b, pl.ds(length, WINDOW)], kvbuf.at[b, pl.ds(0, WINDOW)], hs.at[b], hr.at[b],
                  {"sp": lax.rem(sp + 1, NS)})

    def piece_copy(b, r, src_sp):
        return rc(lst.at[b, r], arr.at[src_sp], asnd.at[b, r], arcv.at[src_sp], {"sp": r * NY + b})

    lane = lax.broadcasted_iota(jnp.int32, (LK, 128), 1)

    @pl.loop(0, NF)
    def _(i):
        b = order(i)

        @pl.when(i == 1)
        def _():
            with scope("h_tok1"):
                token_copy(2).wait_recv()

        @pl.when(i == 2)
        def _():
            with scope("h_tok2"):
                token_copy(3).wait_recv()
            with scope("i_y1"):
                y_arrive(1)

        @pl.when(i == 3)
        def _():
            with scope("h_tok3"):
                token_copy(4).wait_recv()
                token_copy(5).wait_recv()

        p = dot(toks[b], W1[...].reshape(depth, -1)).astype(bf16)
        x = p[:, :LK].astype(f32) + bias[...]
        forget = (jnp.minimum(x, 0.0) - jnp.log1p(jnp.exp(-jnp.abs(x)))) / tau
        hi = forget.astype(bf16)
        f2[b] = jnp.concatenate([hi, (forget - hi.astype(f32)).astype(bf16)], axis=1)
        k = p[:, LK:2 * LK]
        v = p[:, 2 * LK:2 * LK + GLA_VALUE]
        kkey[b] = k
        val[b] = v
        query[b] = p[:, 512:640]
        kvbuf[b, WINDOW:, :] = p[:, 640:]
        faded = (k.astype(f32) * jnp.exp(log_sum(len(levels) + 1, b))).astype(bf16)
        state = dot_rows(faded, v).astype(bf16)
        total = dot_rows(f2[b], jnp.ones((length, 128), bf16))
        decay = jnp.exp(total[:LK] + total[LK:])
        dhi = decay.astype(bf16)
        dlo = (decay - dhi.astype(f32)).astype(bf16)
        packed = jnp.where(lane < 64, dhi.astype(f32), dlo.astype(f32)).astype(bf16)
        lst[b] = jnp.concatenate([state, packed], axis=1).reshape(NZ, RP, GLA_VALUE + 128)

        @pl.loop(0, NZ)
        def _(r):
            @pl.when(r * NY + b != sp)
            def _():
                piece_copy(b, r, sp).start()

            @pl.when(r * NY + b == sp)
            def _():
                arr[sp] = lst[b, r]

        @pl.when(sp < NS - 1)
        def _():
            halo_copy(b).start()

    with scope("i_z2"):
        z_arrive(2)

    @pl.loop(0, NF)
    def _(i):
        b = order(i)

        @pl.when(i == 1)
        def _():
            with scope("i_relay1"):
                relay_arrive(1)

        q = query[b].astype(f32) * LK ** -0.5
        k = kkey[b].astype(f32)
        ri = lax.broadcasted_iota(jnp.int32, (length, length), 0)
        ci = lax.broadcasted_iota(jnp.int32, (length, length), 1)
        rk = lax.broadcasted_iota(jnp.int32, (length, LK), 0)
        scores = jnp.where(ri == ci, dot_t(q.astype(bf16), kkey[b]), 0.0)
        for n, h in enumerate(levels):
            decay = jnp.exp(log_sum(n, b))
            later = (rk & h) != 0
            qh = jnp.where(later, q * decay, 0.0).astype(bf16)
            kh = jnp.where(later, 0.0, k * decay).astype(bf16)
            same = (ri & ~(2 * h - 1)) == (ci & ~(2 * h - 1))
            scores = scores + jnp.where(same, dot_t(qh, kh), 0.0)
        reach[b] = (q * jnp.exp(log_sum(len(levels), b))).astype(bf16)
        oacc[b] = dot(scores.astype(bf16), val[b])

    with scope("k_core1"):
        core_all(1).wait_recv()

    def prefix_copy(s):
        return rc(pre.at[s], state_in.at[yy, zz], qs.at[s], qr.at[sp], {"sp": s})

    def scan():
        def step(s, carry):
            @pl.when(s != sp)
            def _():
                piece_copy(0, 0, s).wait_recv()

            pre[s] = carry.astype(bf16)
            x = arr[s].astype(f32)
            g = x[:, GLA_VALUE:]
            g = g + pltpu.roll(g, 64, 1)
            return carry * jnp.concatenate([g, g], axis=1) + x[:, :GLA_VALUE]

        with scope("l_scan"):
            lax.fori_loop(0, NS, step, jnp.zeros((RP, GLA_VALUE), f32))

        @pl.loop(0, NS)
        def _(s):
            @pl.when(s != sp)
            def _():
                prefix_copy(s).start()

            @pl.when(s == sp)
            def _():
                state_in[yy, zz] = pre[s]

    QB = 64
    row = lax.rem(lax.broadcasted_iota(jnp.int32, (2 * QB, QB + WINDOW), 0), QB)
    col = lax.broadcasted_iota(jnp.int32, (2 * QB, QB + WINDOW), 1)
    band = (col > row) & (col <= row + WINDOW)
    lane_q = lax.broadcasted_iota(jnp.int32, (2 * QB, 128), 1)
    lane_k = lax.broadcasted_iota(jnp.int32, (QB + WINDOW, 128), 1)
    wq = sink.shape[1] * HEAD_DIM

    def rows_copy(src, dst, ssem, rsem, off):
        return rc(src.at[off], dst.at[lax.rem(NF - off, NF)], ssem.at[off], rsem.at[off], at_f(off))

    def wrow_copy(off):
        return rows_copy(wrow, wall, ws, wr, off)

    def lrow_copy(off):
        return rows_copy(lrow, lall, ls, lr, off)

    @pl.loop(0, NF)
    def _(i):
        b = order(i)
        off = lax.rem(b - f + NF, NF)

        @pl.when(i == 1)
        def _():
            with scope("i_owx"):
                for j in range(2):
                    ow_copy(j).wait_recv()
                    ow_copy(4 + j).start()
                    ow_core(j).start()

        @pl.when(i == 2)
        def _():
            scan()

        @pl.when(i == 3)
        def _():
            with scope("m_y2"):
                y_arrive(2)

        @pl.when(sp > 0)
        def _():
            halo_copy(b).wait_recv()

        p = dot(toks[b], W2[...].reshape(depth, -1))
        gates[b] = p[:, wq:].astype(bf16)
        q = (p[:, :wq].astype(bf16).astype(f32) * HEAD_DIM ** -0.5).astype(bf16)
        zero = jnp.zeros((), bf16)
        one = jnp.ones((), bf16)
        blocks = []
        for n in range(length // QB):
            qn = q[n * QB:(n + 1) * QB]
            stacked = jnp.concatenate([qn[:, :128], qn[:, 128:]], axis=0)
            kv = kvbuf[b, n * QB:n * QB + QB + WINDOW, :]
            swapped = jnp.concatenate([kv[:, HEAD_DIM:], kv[:, :HEAD_DIM]], axis=1)
            allowed = band
            if n * QB < WINDOW:
                allowed = band & ((col >= WINDOW - n * QB) | (sp > 0))
            parts, fades = [], []
            for odd in range(2):
                mine = (lane_q >= HEAD_DIM) if odd else (lane_q < HEAD_DIM)
                score = dot_t(jnp.where(mine, stacked, zero), swapped if odd else kv)
                score = jnp.where(allowed, score, -jnp.inf)
                sk = jnp.concatenate([jnp.broadcast_to(sink[0:1, odd:odd + 1], (QB, 1)),
                                      jnp.broadcast_to(sink[0:1, 2 + odd:3 + odd], (QB, 1))], axis=0)
                top = jnp.maximum(jnp.max(score, axis=1, keepdims=True), sk)
                e = jnp.exp(score - top).astype(bf16)
                fades.append(jnp.exp(sk - top))
                ext = jnp.where((lane_k >= HEAD_DIM) if odd else (lane_k < HEAD_DIM), kv if odd else swapped, one)
                parts.append(dot(e, ext))
            low = lane_q < HEAD_DIM
            num = jnp.where(low, parts[0], parts[1])
            den = pltpu.roll(jnp.where(low, parts[1], parts[0]), HEAD_DIM, 1) + jnp.where(low, fades[0], fades[1])
            res = (num / den).astype(bf16)
            blocks.append(jnp.concatenate([res[:QB], res[QB:]], axis=1))
        win = jnp.concatenate(blocks, axis=0)

        @pl.when(i == 0)
        def _():
            wall[0] = win

        @pl.when(i > 0)
        def _():
            wrow[off] = win
            wrow_copy(off).start()

    @pl.loop(0, NF)
    def _(i):
        off = jnp.where(i == 0, 2, jnp.where(i == 1, NF - 1, jnp.where(i == 2, 1, 0)))
        b = lax.rem(f + off, NF)

        with scope("o_state"):
            @pl.loop(0, NZ)
            def _(r):
                o = r * NY + b

                @pl.when(o != sp)
                def _():
                    rc(pre.at[0], state_in.at[b, r], qs.at[0], qr.at[o], {"sp": o}).wait_recv()

        gate = gates[b].astype(f32)
        o = oacc[b] + dot(reach[b], state_in[b].reshape(LK, GLA_VALUE))
        scaled = o * lax.rsqrt(jnp.mean(o * o, axis=1, keepdims=True) + norm_epsilon)
        lin = (scaled * gain[...] * (gate / (1.0 + jnp.exp(-gate)))).astype(bf16)

        @pl.when(off == 0)
        def _():
            lall[0] = lin

        @pl.when(off > 0)
        def _():
            lrow[off] = lin
            lrow_copy(off).start()

    with scope("p_ow"):
        relay_arrive(2)
        for j in range(2, 6):
            ow_copy(j).wait_recv()
            ow_core(j).start()
        ow_core_all().wait_recv()
    with scope("p_wrow"):
        for off in range(1, NF):
            wrow_copy(off).wait_recv()

    chunk = 512

    def out_copy(c):
        cs = pl.ds(c * chunk, chunk)
        return pltpu.make_async_copy(obuf.at[:, cs], out.at[:, cs], lsem.at[9 + c])

    def project(kind, rows_of, init):
        left = jnp.concatenate([rows_of[n] for n in range(NF)], axis=1)
        for c in range(depth // chunk):
            cs = slice(c * chunk, (c + 1) * chunk)
            y = dot(left, OW[kind * NF:(kind + 1) * NF, :, cs].reshape(NF * orows, chunk))
            if init:
                acc[:, cs] = y
            else:
                obuf[:, cs] = (acc[:, cs] + y).astype(bf16)
                out_copy(c).start()

    with scope("q_proj1"):
        project(1, wall, True)
    with scope("r_core2"):
        core_all(2).wait_recv()
    with scope("r_lrow"):
        for off in range(1, NF):
            lrow_copy(off).wait_recv()
    with scope("s_proj2"):
        project(0, lall, False)

    with scope("t_end"):
        for c in range(depth // chunk):
            out_copy(c).wait()
        for j in range(6):
            token_copy(j).wait_send()
            ow_copy(j).wait_send()
        for d in range(1, NF):
            slice_copy(d).wait_send()
            wrow_copy(d).wait_send()
            lrow_copy(d).wait_send()
        for g in range(3):
            for d in range(1, NZ):
                z_copy(g, d).wait_send()
            for k in range(NZ):
                y_copy(g, k, 0).wait_send()
                y_copy(g, k, 1).wait_send()
                relay_copy(g, k).wait_send()
            core_all(g).wait_send()
        ow_core_all().wait_send()

        @pl.when(sp < NS - 1)
        def _():
            for b in range(NF):
                halo_copy(b).wait_send()

        @pl.loop(0, NS)
        def _(s):
            @pl.when(s != sp)
            def _():
                piece_copy(lax.rem(s, NY), s // NY, sp).wait_send()
                prefix_copy(s).wait_send()


def shards(
    NS, NF, NT,
    tokens, linear_query, linear_key, linear_decay, linear_value, linear_gate, decay_bias,
    norm_gain, window_query, window_key, window_value, sink_logit, linear_output, window_output,
):
    _, length, depth = tokens.shape
    kb = linear_query.shape[0]
    NZ = NS // NY
    levels = []
    h = 1
    while h < length:
        levels.append(h)
        h *= 2
    vm = pltpu.VMEM
    dma = pltpu.SemaphoreType.DMA
    kv_width = window_key.shape[1] + window_value.shape[1]
    width1 = 3 * GLA_KEY + GLA_VALUE + kv_width
    width2 = window_query.shape[1] + GLA_VALUE
    anyspec = pl.BlockSpec(memory_space=pl.ANY)
    vspec = pl.BlockSpec(memory_space=vm)
    result = pl.pallas_call(
        functools.partial(kernel, NS, NF, NT, tuple(levels)),
        out_shape=jax.ShapeDtypeStruct((length, depth), bf16),
        in_specs=[anyspec] * 9 + [vspec] * 5,
        out_specs=anyspec,
        scratch_shapes=[
            vm((NF, length, depth), bf16),
            vm((NZ, NY, NT, kb, width1), bf16),
            vm((NZ, NY, NT, kb, width2), bf16),
            vm((2 * NF, linear_output.shape[0], depth), bf16),
            vm((len(levels) + 2, length, length), bf16),
            vm((NF, length, 2 * GLA_KEY), bf16),
            vm((NF, length, GLA_KEY), bf16),
            vm((NF, length, GLA_VALUE), bf16),
            vm((NF, length, GLA_KEY), bf16),
            vm((NF, length + WINDOW, kv_width), bf16),
            vm((NF, NZ, GLA_KEY // NZ, GLA_VALUE + 128), bf16),
            vm((NS, GLA_KEY // NZ, GLA_VALUE + 128), bf16),
            vm((NS, GLA_KEY // NZ, GLA_VALUE), bf16),
            vm((NF, NZ, GLA_KEY // NZ, GLA_VALUE), bf16),
            vm((NF, length, GLA_VALUE), bf16),
            vm((NF, length, window_query.shape[1]), bf16),
            vm((NF, length, GLA_VALUE), bf16),
            vm((NF, length, window_query.shape[1]), bf16),
            vm((NF, length, GLA_VALUE), f32),
            vm((NF, length, GLA_KEY), bf16),
            vm((NF, length, GLA_VALUE), bf16),
            vm((length, depth), f32),
            vm((length, depth), bf16),
            dma((9 + 4,)),
            dma((3, NZ)), dma((3, NZ)),
            dma((3, 2, NZ)), dma((3, 2, NZ)),
            dma((3, NZ)), dma((3, NZ)),
            dma((4,)), dma((4,)),
            dma((6,)), dma((6,)),
            dma((NF,)), dma((NF,)),
            dma((NF, NZ)), dma((NS,)),
            dma((NS,)), dma((NS,)),
            dma((NF,)), dma((NF,)),
            dma((NF,)), dma((NF,)),
            dma((NF,)), dma((NF,)),
            dma((6,)), dma((6,)),
        ],
        compiler_params=pltpu.CompilerParams(
            collective_id=0, has_side_effects=True, vmem_limit_bytes=60 * 1024 * 1024),
        name="layer",
    )(tokens[0], linear_decay, linear_key, linear_value, linear_query, window_query, linear_gate,
      linear_output, window_output, window_key, window_value,
      decay_bias[None], norm_gain[None], sink_logit[None])
    return result[None]


def solution(mesh):
    shape = mesh.shape
    return jax.shard_map(
        functools.partial(shards, shape["sp"], shape["fs"], shape["tp"]),
        mesh=mesh,
        in_specs=(
            P(("fs", "tp"), "sp", None),
            P(("sp", "tp"), "fs"),
            P(("sp", "tp"), "fs"),
            P(("sp", "tp"), "fs"),
            P(("sp", "tp"), "fs"),
            P(("sp", "tp"), "fs"),
            P("fs"),
            P(),
            P(("sp", "tp"), "fs"),
            P(("sp", "tp"), "fs"),
            P(("sp", "tp"), "fs"),
            P("fs"),
            P("fs", None),
            P("fs", None),
        ),
        out_specs=P(("fs", "tp"), "sp", None),
        check_vma=False,
    )
```

```python
import functools

import jax
import jax.numpy as jnp
from jax import lax
from jax.experimental import pallas as pl
from jax.experimental.pallas import tpu as pltpu
from jax.sharding import PartitionSpec as P

GLA_KEY = 128
GLA_VALUE = 256
HEAD_DIM = 64
WINDOW = 128
NY = 4
XR = 128

norm_epsilon = 1e-05
MESH = pl.DeviceIdType.MESH
f32, bf16 = jnp.float32, jnp.bfloat16


def dot(a, b):
    return jnp.dot(a, b, preferred_element_type=f32)


def dot_t(a, b):
    return lax.dot_general(a, b, (((1,), (1,)), ((), ())), preferred_element_type=f32)


def dot_rows(a, b):
    return lax.dot_general(a, b, (((0,), (0,)), ((), ())), preferred_element_type=f32)


def kernel(
    NS, NF, NT, levels,
    tok, w_decay, w_key, w_value, w_lq, w_wq, w_gate, lin_o, win_o, w_wk, w_wv, bias, gain, sink,
    out,
    toks, W1, W2, OW, sums, f2, kkey, val, query, kvbuf, lst, arr, pre, state_in,
    lrow, wrow, lall, wall, oacc, reach, gates, acc, obuf, sc, eb,
    lsem, zs, zr, ys, yr, rr, dsnd, drcv, ts, tr, hs, hr, asnd, arcv, qs, qr,
    ls, lr, ws, wr, xs, xr, os, orr,
):
    sp, f, t = lax.axis_index("sp"), lax.axis_index("fs"), lax.axis_index("tp")
    NZ = NS // NY
    HZ = NZ // 2
    zz, yy = sp // NY, lax.rem(sp, NY)
    length, depth = tok.shape
    half = length // 2
    tau = NS * length // 16
    LK = GLA_KEY
    RP = LK // NZ
    groups = (W1, W2)
    scope = jax.named_scope

    def at_z(d):
        return {"sp": lax.rem(zz + d, NZ) * NY + yy}

    def at_y(d):
        return {"sp": zz * NY + lax.rem(yy + d, NY)}

    def at_f(d):
        return {"fs": lax.rem(f + d, NF)}

    other = {"tp": 1 - t}

    def rc(src, dst, ssem, rsem, dev):
        return pltpu.make_async_remote_copy(
            src_ref=src, dst_ref=dst, send_sem=ssem, recv_sem=rsem, device_id=dev, device_id_type=MESH)

    def got(ref, sem):
        rc(ref, ref, sem, sem, other).wait_recv()

    def gone(ref, sem):
        rc(ref, ref, sem, sem, other).wait_send()

    barrier = pltpu.get_barrier_semaphore()
    greet = [at_z(d) for d in range(1, NZ)] + [at_y(1), at_y(NY - 1)] + [at_f(d) for d in range(1, NF)] + [other]
    for dev in greet:
        pl.semaphore_signal(barrier, inc=1, device_id=dev, device_id_type=MESH)
    own1, own2 = W1.at[zz, yy, t], W2.at[zz, yy, t]
    lin_rows = lin_o.shape[0]
    orows = OW.shape[1]
    loads = [
        (tok, toks.at[f]),
        (w_decay, own1.at[:, 0:128]), (w_key, own1.at[:, 128:256]), (w_value, own1.at[:, 256:512]),
        (w_lq, own1.at[:, 512:640]),
        (w_wq, own2.at[:, 0:256]), (w_gate, own2.at[:, 256:512]),
        (lin_o, OW.at[0, 0:lin_rows]), (win_o, OW.at[0, lin_rows:orows]),
    ]
    local = [pltpu.make_async_copy(a, b, lsem.at[n]) for n, (a, b) in enumerate(loads)]
    for c in local:
        c.start()
    W1[zz, yy, t, :, 640:768] = jnp.concatenate([w_wk[...], w_wv[...]], axis=1)

    i0 = lax.broadcasted_iota(jnp.int32, (length, length), 0)
    s0 = lax.broadcasted_iota(jnp.int32, (length, length), 1)
    for n, h in enumerate(levels):
        ref = (i0 & ~(2 * h - 1)) + h - 1
        later = (i0 & h) != 0
        low = jnp.where(later, ref, i0)
        high = jnp.where(later, i0, ref)
        sums[n] = jnp.where((s0 > low) & (s0 <= high), 1.0, 0.0).astype(bf16)
    sums[len(levels)] = jnp.where(s0 <= i0, 1.0, 0.0).astype(bf16)
    sums[len(levels) + 1] = jnp.where(s0 > i0, 1.0, 0.0).astype(bf16)

    @pl.when(sp == 0)
    def _():
        kvbuf[:, 0:WINDOW, :] = jnp.zeros((NF, WINDOW, kvbuf.shape[2]), bf16)

    with scope("a_loads"):
        for c in local:
            c.wait()
    with scope("b_barrier"):
        pl.semaphore_wait(barrier, len(greet))

    def x_step(j):
        return j in (0, 2, 4), j in (0, 3, 4)

    def token_part(who, first):
        return toks.at[who, pl.ds(0 if first else half, half)]

    def token_send(j):
        right, first = x_step(j)
        who = f if j < 4 else lax.rem(f + (NF - 1 if right else 1), NF)
        ref = token_part(who, first)
        rc(ref, ref, ts.at[0], tr.at[min(j, 4)], at_f(1 if right else NF - 1)).start()

    ocols = depth // NT
    ZR = orows - XR
    cols_t = pl.ds(pl.multiple_of(t * ocols, ocols), ocols)

    def ow_part(rel, first):
        return OW.at[rel, pl.ds(ZR + (0 if first else XR // 2), XR // 2), cols_t]

    def ow_send(j):
        right, first = x_step(j)
        src = 0 if j < 4 else (NF - 1 if right else 1)
        dst = (src + (NF - 1 if right else 1)) % NF
        rc(ow_part(src, first), ow_part(dst, first), os.at[0], orr.at[min(j, 2)],
           at_f(1 if right else NF - 1)).start()

    ow_x = OW.at[pl.ds(1, NF - 1), pl.ds(ZR, XR), cols_t]
    tile_r = ZR // NZ
    tile_c = ocols // NY

    def ow_cols(yo):
        y1 = lax.rem(yy + NY - yo, NY)
        return pl.ds(pl.multiple_of(t * ocols + y1 * tile_c, tile_c), tile_c)

    def ow_rows(z, count):
        return pl.ds(pl.multiple_of(z * tile_r, tile_r), count * tile_r)

    def shard(g, k, yo):
        z1 = lax.rem(zz - k + NZ, NZ)
        if g == 2:
            return OW.at[pl.ds(1, NF - 1), ow_rows(z1, 1), ow_cols(yo)]
        return groups[g].at[z1, lax.rem(yy - yo + NY, NY), t]

    def box(g, z, count, yo):
        if g == 2:
            return OW.at[pl.ds(1, NF - 1), pl.ds(z * tile_r, count * tile_r), ow_cols(yo)]
        return groups[g].at[pl.ds(z, count), lax.rem(yy - yo + NY, NY), t]

    def whole(g, ycount):
        if g == 2:
            return OW.at[pl.ds(1, NF - 1), pl.ds(0, ZR), pl.ds(0, ycount * tile_c)]
        return groups[g].at[:, pl.ds(0, ycount), t]

    pairs = [[0]] + [[d, NZ - d] for d in range(1, HZ)] + [[HZ]]
    ZW = len(pairs)
    zorder = [d for p in pairs[1:] for d in p]
    left, right = 1, NY - 1

    def y_sem(g, side, part):
        return yr.at[side, part if g == 0 else (ZW if g == 1 else ZW + 1 + part)]

    def z_send(g):
        ref = shard(g, 0, 0)
        for p in range(1, ZW):
            for d in pairs[p]:
                rc(ref, ref, zs.at[g], zr.at[p - 1 if g == 0 else ZW - 2 + g], at_z(d)).start()

    def pass_y(g, ref, part):
        rc(ref, ref, ys.at[g], y_sem(g, 0, part), at_y(1)).start()
        rc(ref, ref, ys.at[g], y_sem(g, 1, part), at_y(NY - 1)).start()

    def relay(g, ref, up):
        rc(ref, ref, ys.at[g], rr.at[g], at_y(1 if up else NY - 1)).start()

    def core_send(g, ref):
        rc(ref, ref, dsnd.at[g], drcv.at[g], other).start()

    def core_box(g, yo):
        core_send(g, box(g, 0, NZ, yo))

    def z_arrive(g):
        got(box(g, 0, NZ - 1, 0), zr.at[ZW - 2 + g])
        core_box(g, 0)

    def relay_arrive(g):
        got(box(g, 0, NZ, 2), rr.at[g])
        core_box(g, 2)

    def slice_send(d):
        r, c = ow_rows(zz, 1), ow_cols(0)
        rc(OW.at[0, r, c], OW.at[NF - d, r, c], xs.at[0], xr.at[0], at_f(d)).start()

    slices = OW.at[pl.ds(1, NF - 1), ow_rows(zz, 1), ow_cols(0)]

    for d in range(1, NF):
        slice_send(d)
    z_send(0)
    for j in range(2):
        token_send(j)
    pass_y(0, shard(0, 0, 0), 0)
    for j in range(2, 4):
        token_send(j)
    z_send(1)
    with scope("c_z0"):
        for p in range(1, ZW):
            got(box(0, 0, len(pairs[p]), 0), zr.at[p - 1])
            for k in pairs[p]:
                pass_y(0, shard(0, k, 0), p)
        core_box(0, 0)
    with scope("d_tokfwd"):
        for j in range(2):
            got(token_part(f, True), tr.at[j])
            token_send(4 + j)
    with scope("d_slices"):
        got(slices, xr.at[0])
    z_send(2)
    for j in range(4):
        ow_send(j)
    with scope("e_y0"):
        for p in range(ZW):
            side = p % 2
            got(box(0, 0, len(pairs[p]), 0), y_sem(0, side, p))
            for k in pairs[p]:
                relay(0, shard(0, k, right if side else left), side == 0)
        for p in range(ZW):
            got(box(0, 0, len(pairs[p]), 0), y_sem(0, 1 - p % 2, p))
        core_box(0, left)
        core_box(0, right)
    with scope("e_z1"):
        z_arrive(1)
        pass_y(1, box(1, 0, NZ, 0), 0)
    with scope("f_relay0"):
        relay_arrive(0)
    with scope("g_core0"):
        got(whole(0, NY), drcv.at[0])

    def y_arrive1():
        got(box(1, 0, NZ, 0), y_sem(1, 0, 0))
        relay(1, box(1, 0, HZ, left), True)
        core_box(1, left)
        got(box(1, 0, NZ, 0), y_sem(1, 1, 0))
        relay(1, box(1, HZ, HZ, right), False)
        core_box(1, right)

    def y_arrive2(part):
        if part == 0:
            got(box(2, 0, HZ, 0), y_sem(2, 0, 0))
            relay(2, box(2, 0, HZ, left), True)
            got(box(2, 0, HZ, 0), y_sem(2, 1, 0))
        else:
            got(box(2, 0, HZ, 0), y_sem(2, 1, 1))
            relay(2, box(2, HZ, HZ, right), False)
            got(box(2, 0, HZ, 0), y_sem(2, 0, 1))
            core_box(2, left)
            core_box(2, right)

    def order(i):
        return lax.rem(f + jnp.where(i == 0, 0, jnp.where(i == 1, NF - 1, i - 1)), NF)

    def log_sum(n, b):
        x = dot(sums[n], f2[b])
        return x[:, :LK] + x[:, LK:]

    lane = lax.broadcasted_iota(jnp.int32, (LK, 128), 1)

    @pl.loop(0, NF)
    def _(i):
        b = order(i)

        @pl.when(i == 1)
        def _():
            with scope("h_tok1"):
                got(token_part(f, True), tr.at[2])

        @pl.when(i == 2)
        def _():
            with scope("h_tok2"):
                got(token_part(f, True), tr.at[3])
            with scope("i_y1"):
                y_arrive1()
            with scope("i_z2"):
                z_arrive(2)
                pass_y(2, box(2, 0, HZ, 0), 0)

        @pl.when(i == 3)
        def _():
            with scope("h_tok3"):
                got(toks.at[f], tr.at[4])

        p = dot(toks[b], W1[...].reshape(depth, -1)).astype(bf16)
        x = p[:, :LK].astype(f32) + bias[...]
        forget = (jnp.minimum(x, 0.0) - jnp.log1p(jnp.exp(-jnp.abs(x)))) / tau
        hi = forget.astype(bf16)
        f2[b] = jnp.concatenate([hi, (forget - hi.astype(f32)).astype(bf16)], axis=1)
        k = p[:, LK:2 * LK]
        v = p[:, 2 * LK:2 * LK + GLA_VALUE]
        kkey[b] = k
        val[b] = v
        query[b] = p[:, 512:640]
        kvbuf[b, WINDOW:, :] = p[:, 640:]
        faded = (k.astype(f32) * jnp.exp(log_sum(len(levels) + 1, b))).astype(bf16)
        state = dot_rows(faded, v).astype(bf16)
        total = dot_rows(f2[b], jnp.ones((length, 128), bf16))
        decay = jnp.exp(total[:LK] + total[LK:])
        dhi = decay.astype(bf16)
        dlo = (decay - dhi.astype(f32)).astype(bf16)
        packed = jnp.where(lane < 64, dhi.astype(f32), dlo.astype(f32)).astype(bf16)
        lst[b] = jnp.concatenate([state, packed], axis=1).reshape(NZ, RP, GLA_VALUE + 128)

        @pl.loop(0, NZ)
        def _(r):
            @pl.when(r * NY + b != sp)
            def _():
                rc(lst.at[b, r], arr.at[sp], asnd.at[0], arcv.at[0], {"sp": r * NY + b}).start()

            @pl.when(r * NY + b == sp)
            def _():
                arr[sp] = lst[b, r]

        @pl.when(sp < NS - 1)
        def _():
            rc(kvbuf.at[b, pl.ds(length, WINDOW)], kvbuf.at[b, pl.ds(0, WINDOW)], hs.at[0], hr.at[0],
               {"sp": lax.rem(sp + 1, NS)}).start()

    pass_y(2, box(2, HZ, HZ, 0), 1)

    @pl.loop(0, NF)
    def _(i):
        b = order(i)

        @pl.when(i == 1)
        def _():
            with scope("i_relay1"):
                relay_arrive(1)

        @pl.when(i == 3)
        def _():
            with scope("i_y2"):
                y_arrive2(0)

        q = query[b].astype(f32) * LK ** -0.5
        k = kkey[b].astype(f32)
        ri = lax.broadcasted_iota(jnp.int32, (length, length), 0)
        ci = lax.broadcasted_iota(jnp.int32, (length, length), 1)
        rk = lax.broadcasted_iota(jnp.int32, (length, LK), 0)
        scores = jnp.where(ri == ci, dot_t(q.astype(bf16), kkey[b]), 0.0)
        for n, h in enumerate(levels):
            decay = jnp.exp(log_sum(n, b))
            later = (rk & h) != 0
            qh = jnp.where(later, q * decay, 0.0).astype(bf16)
            kh = jnp.where(later, 0.0, k * decay).astype(bf16)
            same = (ri & ~(2 * h - 1)) == (ci & ~(2 * h - 1))
            scores = scores + jnp.where(same, dot_t(qh, kh), 0.0)
        reach[b] = (q * jnp.exp(log_sum(len(levels), b))).astype(bf16)
        oacc[b] = dot(scores.astype(bf16), val[b])

    with scope("k_core1"):
        got(whole(1, NY), drcv.at[1])
    with scope("i_owx"):
        for j in range(2):
            got(ow_part(0, True), orr.at[j])
            ow_send(4 + j)

    def scan():
        with scope("l_scan"):
            got(arr.at[pl.ds(0, NS - 1)], arcv.at[0])

        unroll = 8

        def step(n, carry):
            for m in range(unroll):
                s = n * unroll + m
                pre[s] = carry.astype(bf16)
                x = arr[s].astype(f32)
                g = x[:, GLA_VALUE:]
                g = g + pltpu.roll(g, 64, 1)
                carry = carry * jnp.concatenate([g, g], axis=1) + x[:, :GLA_VALUE]
            return carry

        with scope("l_scan2"):
            lax.fori_loop(0, NS // unroll, step, jnp.zeros((RP, GLA_VALUE), f32))
            state_in[yy, zz] = pre[sp]

            @pl.loop(1, NS)
            def _(n):
                s = lax.rem(sp + n, NS)
                rc(pre.at[s], state_in.at[yy, zz], qs.at[0], qr.at[yy], {"sp": s}).start()

    QB = 64
    units = 2 * (length // QB)
    row = lax.rem(lax.broadcasted_iota(jnp.int32, (2 * QB, QB + WINDOW), 0), QB)
    col = lax.broadcasted_iota(jnp.int32, (2 * QB, QB + WINDOW), 1)
    band = (col > row) & (col <= row + WINDOW)
    lane_q = lax.broadcasted_iota(jnp.int32, (2 * QB, 128), 1)
    lane_k = lax.broadcasted_iota(jnp.int32, (QB + WINDOW, 128), 1)
    row_k = lax.broadcasted_iota(jnp.int32, (QB + WINDOW, 128), 0)
    wq = sink.shape[1] * HEAD_DIM

    def rows_send(src, dst, ssem, rsem, off):
        rc(src.at[off], dst.at[lax.rem(NF - off, NF)], ssem.at[0], rsem.at[0], at_f(off)).start()

    @pl.when(sp > 0)
    def _():
        with scope("k_halo"):
            got(kvbuf.at[:, pl.ds(0, WINDOW)], hr.at[0])

    @pl.loop(0, NF)
    def _(i):
        b = order(i)
        off = lax.rem(b - f + NF, NF)

        @pl.when(i == 2)
        def _():
            scan()

        @pl.when(i == 3)
        def _():
            with scope("m_y2"):
                y_arrive2(1)

        p = dot(toks[b], W2[...].reshape(depth, -1))
        gates[b] = p[:, wq:].astype(bf16)
        q = (p[:, :wq].astype(bf16).astype(f32) * HEAD_DIM ** -0.5).astype(bf16)
        zero = jnp.zeros((), bf16)
        one = jnp.ones((), bf16)

        def keys(n):
            kv = kvbuf[b, n * QB:n * QB + QB + WINDOW, :]
            return kv, jnp.concatenate([kv[:, HEAD_DIM:], kv[:, :HEAD_DIM]], axis=1)

        for n in range(length // QB):
            qn = q[n * QB:(n + 1) * QB]
            stacked = jnp.concatenate([qn[:, :128], qn[:, 128:]], axis=0)
            kv, swapped = keys(n)
            allowed = band
            if n * QB < WINDOW:
                allowed = band & ((col >= WINDOW - n * QB) | (sp > 0))
            for odd in range(2):
                mine = (lane_q >= HEAD_DIM) if odd else (lane_q < HEAD_DIM)
                score = dot_t(jnp.where(mine, stacked, zero), swapped if odd else kv)
                sk = jnp.concatenate([jnp.broadcast_to(sink[0:1, odd:odd + 1], (QB, 1)),
                                      jnp.broadcast_to(sink[0:1, 2 + odd:3 + odd], (QB, 1))], axis=0)
                sc[2 * n + odd] = jnp.where(allowed, score, jnp.where(col == 0, sk, -jnp.inf))
        for u in range(units):
            score = sc[u]
            eb[u] = jnp.exp(score - jnp.max(score, axis=1, keepdims=True)).astype(bf16)
        blocks = []
        for n in range(length // QB):
            kv, swapped = keys(n)
            parts = []
            for odd in range(2):
                vals = jnp.where(row_k == 0, zero, kv if odd else swapped)
                ext = jnp.where((lane_k >= HEAD_DIM) if odd else (lane_k < HEAD_DIM), vals, one)
                parts.append(dot(eb[2 * n + odd], ext))
            low = lane_q < HEAD_DIM
            num = jnp.where(low, parts[0], parts[1])
            den = pltpu.roll(jnp.where(low, parts[1], parts[0]), HEAD_DIM, 1)
            res = (num / den).astype(bf16)
            blocks.append(jnp.concatenate([res[:QB], res[QB:]], axis=1))
        win = jnp.concatenate(blocks, axis=0)

        @pl.when(i == 0)
        def _():
            wall[0] = win

        @pl.when(i > 0)
        def _():
            wrow[off] = win
            rows_send(wrow, wall, ws, wr, off)

    with scope("n_ow"):
        relay_arrive(2)
        got(OW.at[pl.ds(1, 2), pl.ds(ZR, XR), cols_t], orr.at[2])
        core_send(3, ow_x)

    @pl.loop(0, NF)
    def _(i):
        off = jnp.where(i == 0, 2, jnp.where(i == 1, NF - 1, jnp.where(i == 2, 1, 0)))
        b = lax.rem(f + off, NF)

        with scope("o_state"):
            @pl.when(b != yy)
            def _():
                got(state_in.at[b], qr.at[b])

            @pl.when(b == yy)
            def _():
                got(state_in.at[b, pl.ds(0, NZ - 1)], qr.at[b])

        gate = gates[b].astype(f32)
        o = oacc[b] + dot(reach[b], state_in[b].reshape(LK, GLA_VALUE))
        scaled = o * lax.rsqrt(jnp.mean(o * o, axis=1, keepdims=True) + norm_epsilon)
        lin = (scaled * gain[...] * (gate / (1.0 + jnp.exp(-gate)))).astype(bf16)

        @pl.when(off == 0)
        def _():
            lall[0] = lin

        @pl.when(off > 0)
        def _():
            lrow[off] = lin
            rows_send(lrow, lall, ls, lr, off)

    with scope("p_ow"):
        got(whole(2, NY), drcv.at[2])
        got(ow_x, drcv.at[3])
    with scope("p_wrow"):
        got(wall.at[pl.ds(1, NF - 1)], wr.at[0])

    chunk = 512

    def out_copy(c):
        cs = pl.ds(c * chunk, chunk)
        return pltpu.make_async_copy(obuf.at[:, cs], out.at[:, cs], lsem.at[c])

    def project(lo, hi, rows_of, init):
        lhs = jnp.concatenate([rows_of[n] for n in range(NF)], axis=1)
        for c in range(depth // chunk):
            cs = slice(c * chunk, (c + 1) * chunk)
            y = dot(lhs, OW[:, lo:hi, cs].reshape(-1, chunk))
            if init:
                acc[:, cs] = y
            else:
                obuf[:, cs] = (acc[:, cs] + y).astype(bf16)
                out_copy(c).start()

    with scope("q_proj1"):
        project(lin_rows, orows, wall, True)
    with scope("r_lrow"):
        got(lall.at[pl.ds(1, NF - 1)], lr.at[0])
    with scope("s_proj2"):
        project(0, lin_rows, lall, False)

    with scope("t_end"):
        gone(toks.at[pl.ds(0, NF - 1)], ts.at[0])
        gone(ow_x, os.at[0])
        gone(slices, xs.at[0])
        gone(wrow.at[pl.ds(1, NF - 1)], ws.at[0])
        gone(lrow.at[pl.ds(1, NF - 1)], ls.at[0])
        for g in range(3):
            gone(box(g, 0, NZ - 1, 0), zs.at[g])
            gone(whole(g, 3), ys.at[g])
            gone(whole(g, NY), dsnd.at[g])
        gone(ow_x, dsnd.at[3])
        gone(arr.at[pl.ds(0, NS - 1)], asnd.at[0])
        gone(pre.at[pl.ds(0, NS - 1)], qs.at[0])

        @pl.when(sp < NS - 1)
        def _():
            gone(kvbuf.at[:, pl.ds(0, WINDOW)], hs.at[0])

        for c in range(depth // chunk):
            out_copy(c).wait()


def shards(
    NS, NF, NT,
    tokens, linear_query, linear_key, linear_decay, linear_value, linear_gate, decay_bias,
    norm_gain, window_query, window_key, window_value, sink_logit, linear_output, window_output,
):
    _, length, depth = tokens.shape
    kb = linear_query.shape[0]
    NZ = NS // NY
    levels = []
    h = 1
    while h < length:
        levels.append(h)
        h *= 2
    vm = pltpu.VMEM
    dma = pltpu.SemaphoreType.DMA
    kv_width = window_key.shape[1] + window_value.shape[1]
    width1 = 3 * GLA_KEY + GLA_VALUE + kv_width
    width2 = window_query.shape[1] + GLA_VALUE
    anyspec = pl.BlockSpec(memory_space=pl.ANY)
    vspec = pl.BlockSpec(memory_space=vm)
    result = pl.pallas_call(
        functools.partial(kernel, NS, NF, NT, tuple(levels)),
        out_shape=jax.ShapeDtypeStruct((length, depth), bf16),
        in_specs=[anyspec] * 9 + [vspec] * 5,
        out_specs=anyspec,
        scratch_shapes=[
            vm((NF, length, depth), bf16),
            vm((NZ, NY, NT, kb, width1), bf16),
            vm((NZ, NY, NT, kb, width2), bf16),
            vm((NF, linear_output.shape[0] + window_output.shape[0], depth), bf16),
            vm((len(levels) + 2, length, length), bf16),
            vm((NF, length, 2 * GLA_KEY), bf16),
            vm((NF, length, GLA_KEY), bf16),
            vm((NF, length, GLA_VALUE), bf16),
            vm((NF, length, GLA_KEY), bf16),
            vm((NF, length + WINDOW, kv_width), bf16),
            vm((NF, NZ, GLA_KEY // NZ, GLA_VALUE + 128), bf16),
            vm((NS, GLA_KEY // NZ, GLA_VALUE + 128), bf16),
            vm((NS, GLA_KEY // NZ, GLA_VALUE), bf16),
            vm((NF, NZ, GLA_KEY // NZ, GLA_VALUE), bf16),
            vm((NF, length, GLA_VALUE), bf16),
            vm((NF, length, window_query.shape[1]), bf16),
            vm((NF, length, GLA_VALUE), bf16),
            vm((NF, length, window_query.shape[1]), bf16),
            vm((NF, length, GLA_VALUE), f32),
            vm((NF, length, GLA_KEY), bf16),
            vm((NF, length, GLA_VALUE), bf16),
            vm((length, depth), f32),
            vm((length, depth), bf16),
            vm((6, 128, 192), f32),
            vm((6, 128, 192), bf16),
            dma((9,)),
            dma((3,)), dma((NZ // 2 + 2,)),
            dma((3,)), dma((2, NZ // 2 + 4)),
            dma((3,)),
            dma((4,)), dma((4,)),
            dma((1,)), dma((5,)),
            dma((1,)), dma((1,)),
            dma((1,)), dma((1,)),
            dma((1,)), dma((NF,)),
            dma((1,)), dma((1,)),
            dma((1,)), dma((1,)),
            dma((1,)), dma((1,)),
            dma((1,)), dma((3,)),
        ],
        compiler_params=pltpu.CompilerParams(
            collective_id=0, has_side_effects=True, vmem_limit_bytes=60 * 1024 * 1024),
        name="layer",
    )(tokens[0], linear_decay, linear_key, linear_value, linear_query, window_query, linear_gate,
      linear_output, window_output, window_key, window_value,
      decay_bias[None], norm_gain[None], sink_logit[None])
    return result[None]


def solution(mesh):
    shape = mesh.shape
    return jax.shard_map(
        functools.partial(shards, shape["sp"], shape["fs"], shape["tp"]),
        mesh=mesh,
        in_specs=(
            P(("fs", "tp"), "sp", None),
            P(("sp", "tp"), "fs"),
            P(("sp", "tp"), "fs"),
            P(("sp", "tp"), "fs"),
            P(("sp", "tp"), "fs"),
            P(("sp", "tp"), "fs"),
            P("fs"),
            P(),
            P(("sp", "tp"), "fs"),
            P(("sp", "tp"), "fs"),
            P(("sp", "tp"), "fs"),
            P("fs"),
            P("fs", None),
            P("fs", None),
        ),
        out_specs=P(("fs", "tp"), "sp", None),
        check_vma=False,
    )
```

```python
import functools

import jax
import jax.numpy as jnp
from jax import lax
from jax.experimental import pallas as pl
from jax.experimental.pallas import tpu as pltpu
from jax.sharding import PartitionSpec as P

GLA_KEY = 128
GLA_VALUE = 256
HEAD_DIM = 64
WINDOW = 128
NY = 4
XR = 128
ZF = 128

norm_epsilon = 1e-05
MESH = pl.DeviceIdType.MESH
f32, bf16 = jnp.float32, jnp.bfloat16


def dot(a, b):
    return jnp.dot(a, b, preferred_element_type=f32)


def dot_t(a, b):
    return lax.dot_general(a, b, (((1,), (1,)), ((), ())), preferred_element_type=f32)


def dot_rows(a, b):
    return lax.dot_general(a, b, (((0,), (0,)), ((), ())), preferred_element_type=f32)


def kernel(
    NS, NF, NT, levels,
    tok, w_decay, w_key, w_value, w_lq, w_wq, w_gate, lin_o, win_o, w_wk, w_wv, bias, gain, sink,
    out,
    toks, W1, W2, OW, sums, f2, kkey, val, query, kvbuf, lst, arr, pre, state_in,
    lrow, wrow, lall, wall, oacc, reach, gates, acc, obuf, sc, eb,
    lsem, zs, zr, zrr, ys, yr, rr, dsnd, drcv, ts, tr, hs, hr, asnd, arcv, qs, qr,
    ls, lr, ws, wr, xs, xr, os, orr,
):
    sp, f, t = lax.axis_index("sp"), lax.axis_index("fs"), lax.axis_index("tp")
    NZ = NS // NY
    HZ = NZ // 2
    zz, yy = sp // NY, lax.rem(sp, NY)
    length, depth = tok.shape
    half = length // 2
    tau = NS * length // 16
    LK = GLA_KEY
    RP = LK // NZ
    groups = (W1, W2)
    scope = jax.named_scope

    def at_z(d):
        return {"sp": lax.rem(zz + d, NZ) * NY + yy}

    def at_y(d):
        return {"sp": zz * NY + lax.rem(yy + d, NY)}

    def at_f(d):
        return {"fs": lax.rem(f + d, NF)}

    other = {"tp": 1 - t}

    def rc(src, dst, ssem, rsem, dev):
        return pltpu.make_async_remote_copy(
            src_ref=src, dst_ref=dst, send_sem=ssem, recv_sem=rsem, device_id=dev, device_id_type=MESH)

    def got(ref, sem):
        rc(ref, ref, sem, sem, other).wait_recv()

    def gone(ref, sem):
        rc(ref, ref, sem, sem, other).wait_send()

    barrier = pltpu.get_barrier_semaphore()
    greet = [at_z(d) for d in range(1, NZ)] + [at_y(d) for d in range(1, NY)] + [at_f(d) for d in range(1, NF)] + [other]
    for dev in greet:
        pl.semaphore_signal(barrier, inc=1, device_id=dev, device_id_type=MESH)
    own1, own2 = W1.at[zz, yy, t], W2.at[zz, yy, t]
    lin_rows = lin_o.shape[0]
    orows = OW.shape[1]
    loads = [
        (tok, toks.at[f]),
        (w_decay, own1.at[:, 0:128]), (w_key, own1.at[:, 128:256]), (w_value, own1.at[:, 256:512]),
        (w_lq, own1.at[:, 512:640]),
        (w_wq, own2.at[:, 0:256]), (w_gate, own2.at[:, 256:512]),
        (lin_o, OW.at[0, 0:lin_rows]), (win_o, OW.at[0, lin_rows:orows]),
    ]
    local = [pltpu.make_async_copy(a, b, lsem.at[n]) for n, (a, b) in enumerate(loads)]
    for c in local:
        c.start()
    W1[zz, yy, t, :, 640:768] = jnp.concatenate([w_wk[...], w_wv[...]], axis=1)

    i0 = lax.broadcasted_iota(jnp.int32, (length, length), 0)
    s0 = lax.broadcasted_iota(jnp.int32, (length, length), 1)
    for n, h in enumerate(levels):
        ref = (i0 & ~(2 * h - 1)) + h - 1
        later = (i0 & h) != 0
        low = jnp.where(later, ref, i0)
        high = jnp.where(later, i0, ref)
        sums[n] = jnp.where((s0 > low) & (s0 <= high), 1.0, 0.0).astype(bf16)
    sums[len(levels)] = jnp.where(s0 <= i0, 1.0, 0.0).astype(bf16)
    sums[len(levels) + 1] = jnp.where(s0 > i0, 1.0, 0.0).astype(bf16)

    @pl.when(sp == 0)
    def _():
        kvbuf[:, 0:WINDOW, :] = jnp.zeros((NF, WINDOW, kvbuf.shape[2]), bf16)

    with scope("a_loads"):
        for c in local[:7]:
            c.wait()
    with scope("b_barrier"):
        pl.semaphore_wait(barrier, len(greet))

    def x_step(j):
        return j in (0, 2, 4), j in (0, 3, 4)

    def token_part(who, first):
        return toks.at[who, pl.ds(0 if first else half, half)]

    def token_send(j):
        right, first = x_step(j)
        who = f if j < 4 else lax.rem(f + (NF - 1 if right else 1), NF)
        ref = token_part(who, first)
        rc(ref, ref, ts.at[0], tr.at[min(j, 4)], at_f(1 if right else NF - 1)).start()

    ocols = depth // NT
    ZR = orows - XR
    cols_t = pl.ds(pl.multiple_of(t * ocols, ocols), ocols)

    def ow_part(rel, first):
        return OW.at[rel, pl.ds(ZR + (0 if first else XR // 2), XR // 2), cols_t]

    def ow_send(j):
        right, first = x_step(j)
        src = 0 if j < 4 else (NF - 1 if right else 1)
        dst = (src + (NF - 1 if right else 1)) % NF
        rc(ow_part(src, first), ow_part(dst, first), os.at[0], orr.at[min(j, 2)],
           at_f(1 if right else NF - 1)).start()

    tile_c = ocols // NY
    region = {2: (ZR - ZF, ZF // NZ), 3: (0, (ZR - ZF) // NZ)}
    others = pl.ds(1, NF - 1)
    ow_x = OW.at[others, pl.ds(ZR, XR), cols_t]

    def ow_cols(yo):
        y1 = lax.rem(yy + NY - yo, NY)
        return pl.ds(pl.multiple_of(t * ocols + y1 * tile_c, tile_c), tile_c)

    def ow_rows(g, z, count):
        first, tile = region[g]
        start = first + z * tile
        return pl.ds(start if isinstance(z, int) else pl.multiple_of(start, tile), count * tile)

    def shard(g, k, yo):
        z1 = lax.rem(zz - k + NZ, NZ)
        if g == 2:
            return OW.at[others, ow_rows(2, z1, 1), ow_cols(yo)]
        return groups[g].at[z1, lax.rem(yy - yo + NY, NY), t]

    def box(g, z, count, yo):
        if g == 2:
            return OW.at[others, ow_rows(2, z, count), ow_cols(yo)]
        return groups[g].at[pl.ds(z, count), lax.rem(yy - yo + NY, NY), t]

    def whole(g, ycount):
        if g == 2:
            return OW.at[others, ow_rows(2, 0, NZ), pl.ds(0, ycount * tile_c)]
        return groups[g].at[:, pl.ds(0, ycount), t]

    pairs = [[0]] + [[d, NZ - d] for d in range(1, HZ)] + [[HZ]]
    ZW = len(pairs)
    zorder = [d for p in pairs[1:] for d in p]
    left, right = 1, NY - 1

    def y_sem(g, side, part):
        return yr.at[side, part if g == 0 else ZW + g]

    def z_send(g):
        ref = shard(g, 0, 0)
        for p in range(1, ZW):
            for d in pairs[p]:
                rc(ref, ref, zs.at[g], zr.at[p - 1 if g == 0 else ZW - 2 + g], at_z(d)).start()

    def pass_y(g, ref, part):
        rc(ref, ref, ys.at[g], y_sem(g, 0, part), at_y(1)).start()
        rc(ref, ref, ys.at[g], y_sem(g, 1, part), at_y(NY - 1)).start()

    def relay(g, ref, up):
        rc(ref, ref, ys.at[g], rr.at[g], at_y(1 if up else NY - 1)).start()

    def core_send(g, ref):
        rc(ref, ref, dsnd.at[g], drcv.at[g], other).start()

    def core_box(g, yo):
        core_send(g, box(g, 0, NZ, yo))

    def z_arrive(g):
        got(box(g, 0, NZ - 1, 0), zr.at[ZW - 2 + g])
        core_box(g, 0)

    def relay_arrive(g):
        got(box(g, 0, NZ, 2), rr.at[g])
        core_box(g, 2)

    def slice_send(g, d):
        r, c = ow_rows(g, zz, 1), ow_cols(0)
        src = lin_o if g == 3 else win_o
        r0 = pl.ds(pl.multiple_of(zz * region[g][1], region[g][1]), region[g][1])
        rc(src.at[r0, c], OW.at[NF - d, r, c], xs.at[g - 2], xr.at[g - 2], at_f(d)).start()

    def slices(g):
        return OW.at[others, ow_rows(g, zz, 1), ow_cols(0)]

    def ring_block(d):
        return OW.at[others, ow_rows(3, lax.rem(zz + d + NZ, NZ), 1), cols_t]

    def ring_half(d, up):
        cols = pl.ds(pl.multiple_of(t * ocols + (0 if up else ocols // 2), ocols // 2), ocols // 2)
        return OW.at[others, ow_rows(3, lax.rem(zz + d + NZ, NZ), 1), cols]

    def ring_spread():
        ref = slices(3)
        for d in range(1, NY):
            rc(ref, ref, ys.at[3], yr.at[0, ZW], at_y(d)).start()

    def ring_ref(s, up):
        d = -s if up else s
        return ring_half(d, up) if s == HZ - 1 else ring_block(d)

    def ring_step(s):
        if s == 0:
            got(OW.at[others, ow_rows(3, zz, 1), pl.ds(0, (NY - 1) * tile_c)], yr.at[0, ZW])
            core_send(4, ring_block(0))
        for up in (True, False):
            if s > 0:
                got(ring_ref(s - 1, up), zrr.at[0 if up else 1, s - 1])
            if s < HZ:
                ref = ring_ref(s, up)
                rc(ref, ref, zs.at[3], zrr.at[0 if up else 1, s], at_z(1 if up else NZ - 1)).start()
            if 0 < s < HZ:
                core_send(4, ring_block(-s if up else s))
        if s == HZ:
            core_send(4, ring_block(HZ))

    ring_all = OW.at[others, ow_rows(3, 0, NZ), cols_t]

    for g in (3, 2):
        for d in range(1, NF):
            slice_send(g, d)
    z_send(0)
    for j in range(2):
        token_send(j)
    pass_y(0, shard(0, 0, 0), 0)
    for j in range(2, 4):
        token_send(j)
    z_send(1)
    with scope("c_slices"):
        got(slices(3), xr.at[1])
        ring_spread()
    with scope("c_z0"):
        for p in range(1, ZW):
            got(box(0, 0, len(pairs[p]), 0), zr.at[p - 1])
            for k in pairs[p]:
                pass_y(0, shard(0, k, 0), p)
        core_box(0, 0)
    with scope("d_tokfwd"):
        for j in range(2):
            got(token_part(f, True), tr.at[j])
            token_send(4 + j)
    with scope("d_ring0"):
        ring_step(0)
        got(slices(2), xr.at[0])
    z_send(2)
    for c in local[7:]:
        c.wait()
    for j in range(4):
        ow_send(j)
    with scope("e_y0"):
        for p in range(ZW):
            side = p % 2
            got(box(0, 0, len(pairs[p]), 0), y_sem(0, side, p))
            for k in pairs[p]:
                relay(0, shard(0, k, right if side else left), side == 0)
        for p in range(ZW):
            got(box(0, 0, len(pairs[p]), 0), y_sem(0, 1 - p % 2, p))
        core_box(0, left)
        core_box(0, right)
    with scope("e_z1"):
        z_arrive(1)
        pass_y(1, box(1, 0, NZ, 0), 0)
    with scope("f_relay0"):
        relay_arrive(0)
    with scope("g_core0"):
        got(whole(0, NY), drcv.at[0])

    def y_arrive(g):
        got(box(g, 0, NZ, 0), y_sem(g, 0, 0))
        relay(g, box(g, 0, HZ, left), True)
        core_box(g, left)
        got(box(g, 0, NZ, 0), y_sem(g, 1, 0))
        relay(g, box(g, HZ, HZ, right), False)
        core_box(g, right)

    def order(i):
        return lax.rem(f + jnp.where(i == 0, 0, jnp.where(i == 1, NF - 1, i - 1)), NF)

    def log_sum(n, b):
        x = dot(sums[n], f2[b])
        return x[:, :LK] + x[:, LK:]

    lane = lax.broadcasted_iota(jnp.int32, (LK, 128), 1)

    def intra(b):
        q = query[b].astype(f32) * LK ** -0.5
        k = kkey[b].astype(f32)
        ri = lax.broadcasted_iota(jnp.int32, (length, length), 0)
        ci = lax.broadcasted_iota(jnp.int32, (length, length), 1)
        rk = lax.broadcasted_iota(jnp.int32, (length, LK), 0)
        scores = jnp.where(ri == ci, dot_t(q.astype(bf16), kkey[b]), 0.0)
        for n, h in enumerate(levels):
            decay = jnp.exp(log_sum(n, b))
            later = (rk & h) != 0
            qh = jnp.where(later, q * decay, 0.0).astype(bf16)
            kh = jnp.where(later, 0.0, k * decay).astype(bf16)
            same = (ri & ~(2 * h - 1)) == (ci & ~(2 * h - 1))
            scores = scores + jnp.where(same, dot_t(qh, kh), 0.0)
        reach[b] = (q * jnp.exp(log_sum(len(levels), b))).astype(bf16)
        oacc[b] = dot(scores.astype(bf16), val[b])

    @pl.loop(0, NF)
    def _(i):
        b = order(i)

        @pl.when(i == 1)
        def _():
            with scope("h_tok1"):
                got(token_part(f, True), tr.at[2])
            with scope("h_ring1"):
                ring_step(1)

        @pl.when(i == 2)
        def _():
            with scope("h_tok2"):
                got(token_part(f, True), tr.at[3])
            with scope("i_y1"):
                y_arrive(1)
            with scope("i_z2"):
                z_arrive(2)
                pass_y(2, box(2, 0, NZ, 0), 0)

        @pl.when(i == 3)
        def _():
            intra(f)
            with scope("h_tok3"):
                got(toks.at[f], tr.at[4])

        p = dot(toks[b], W1[...].reshape(depth, -1)).astype(bf16)
        x = p[:, :LK].astype(f32) + bias[...]
        forget = (jnp.minimum(x, 0.0) - jnp.log1p(jnp.exp(-jnp.abs(x)))) / tau
        hi = forget.astype(bf16)
        f2[b] = jnp.concatenate([hi, (forget - hi.astype(f32)).astype(bf16)], axis=1)
        k = p[:, LK:2 * LK]
        v = p[:, 2 * LK:2 * LK + GLA_VALUE]
        kkey[b] = k
        val[b] = v
        query[b] = p[:, 512:640]
        kvbuf[b, WINDOW:, :] = p[:, 640:]
        faded = (k.astype(f32) * jnp.exp(log_sum(len(levels) + 1, b))).astype(bf16)
        state = dot_rows(faded, v).astype(bf16)
        total = dot_rows(f2[b], jnp.ones((length, 128), bf16))
        decay = jnp.exp(total[:LK] + total[LK:])
        dhi = decay.astype(bf16)
        dlo = (decay - dhi.astype(f32)).astype(bf16)
        packed = jnp.where(lane < 64, dhi.astype(f32), dlo.astype(f32)).astype(bf16)
        lst[b] = jnp.concatenate([state, packed], axis=1).reshape(NZ, RP, GLA_VALUE + 128)

        @pl.loop(0, NZ)
        def _(r):
            @pl.when(r * NY + b != sp)
            def _():
                rc(lst.at[b, r], arr.at[sp], asnd.at[0], arcv.at[0], {"sp": r * NY + b}).start()

            @pl.when(r * NY + b == sp)
            def _():
                arr[sp] = lst[b, r]

        @pl.when(sp < NS - 1)
        def _():
            rc(kvbuf.at[b, pl.ds(length, WINDOW)], kvbuf.at[b, pl.ds(0, WINDOW)], hs.at[0], hr.at[b],
               {"sp": lax.rem(sp + 1, NS)}).start()

    @pl.loop(1, NF)
    def _(i):
        @pl.when(i == 2)
        def _():
            with scope("i_relay1"):
                relay_arrive(1)

        @pl.when(i == 3)
        def _():
            with scope("h_ring2"):
                ring_step(2)

        intra(order(i))

    with scope("k_core1"):
        got(whole(1, NY), drcv.at[1])
    with scope("i_owx"):
        for j in range(2):
            got(ow_part(0, True), orr.at[j])
            ow_send(4 + j)

    def scan():
        with scope("l_scan"):
            got(arr.at[pl.ds(0, NS - 1)], arcv.at[0])

        unroll = 8

        def step(n, carry):
            for m in range(unroll):
                s = n * unroll + m
                pre[s] = carry.astype(bf16)
                x = arr[s].astype(f32)
                g = x[:, GLA_VALUE:]
                g = g + pltpu.roll(g, 64, 1)
                carry = carry * jnp.concatenate([g, g], axis=1) + x[:, :GLA_VALUE]
            return carry

        with scope("l_scan2"):
            lax.fori_loop(0, NS // unroll, step, jnp.zeros((RP, GLA_VALUE), f32))
            state_in[yy, zz] = pre[sp]

            @pl.loop(1, NS)
            def _(n):
                s = lax.rem(sp + n, NS)
                rc(pre.at[s], state_in.at[yy, zz], qs.at[0], qr.at[yy], {"sp": s}).start()

    QB = 64
    units = 2 * (length // QB)
    row = lax.rem(lax.broadcasted_iota(jnp.int32, (2 * QB, QB + WINDOW), 0), QB)
    col = lax.broadcasted_iota(jnp.int32, (2 * QB, QB + WINDOW), 1)
    band = (col > row) & (col <= row + WINDOW)
    lane_q = lax.broadcasted_iota(jnp.int32, (2 * QB, 128), 1)
    lane_k = lax.broadcasted_iota(jnp.int32, (QB + WINDOW, 128), 1)
    row_k = lax.broadcasted_iota(jnp.int32, (QB + WINDOW, 128), 0)
    wq = sink.shape[1] * HEAD_DIM

    def rows_send(src, dst, ssem, rsem, off):
        rc(src.at[off], dst.at[lax.rem(NF - off, NF)], ssem.at[0], rsem.at[0], at_f(off)).start()

    @pl.loop(0, NF)
    def _(i):
        off = jnp.where(i == 0, NF - 1, jnp.where(i == NF - 1, 0, i))
        b = lax.rem(f + off, NF)

        @pl.when(i == 2)
        def _():
            scan()

        @pl.when(i == 3)
        def _():
            with scope("m_y2"):
                y_arrive(2)
            with scope("m_ring3"):
                ring_step(3)

        @pl.when(sp > 0)
        def _():
            with scope("k_halo"):
                got(kvbuf.at[b, pl.ds(0, WINDOW)], hr.at[b])

        p = dot(toks[b], W2[...].reshape(depth, -1))
        gates[b] = p[:, wq:].astype(bf16)
        q = (p[:, :wq].astype(bf16).astype(f32) * HEAD_DIM ** -0.5).astype(bf16)
        zero = jnp.zeros((), bf16)
        one = jnp.ones((), bf16)

        def keys(n):
            kv = kvbuf[b, n * QB:n * QB + QB + WINDOW, :]
            return kv, jnp.concatenate([kv[:, HEAD_DIM:], kv[:, :HEAD_DIM]], axis=1)

        for n in range(length // QB):
            qn = q[n * QB:(n + 1) * QB]
            stacked = jnp.concatenate([qn[:, :128], qn[:, 128:]], axis=0)
            kv, swapped = keys(n)
            allowed = band
            if n * QB < WINDOW:
                allowed = band & ((col >= WINDOW - n * QB) | (sp > 0))
            for odd in range(2):
                mine = (lane_q >= HEAD_DIM) if odd else (lane_q < HEAD_DIM)
                score = dot_t(jnp.where(mine, stacked, zero), swapped if odd else kv)
                sk = jnp.concatenate([jnp.broadcast_to(sink[0:1, odd:odd + 1], (QB, 1)),
                                      jnp.broadcast_to(sink[0:1, 2 + odd:3 + odd], (QB, 1))], axis=0)
                sc[2 * n + odd] = jnp.where(allowed, score, jnp.where(col == 0, sk, -jnp.inf))
        for u in range(units):
            score = sc[u]
            eb[u] = jnp.exp(score - jnp.max(score, axis=1, keepdims=True)).astype(bf16)
        blocks = []
        for n in range(length // QB):
            kv, swapped = keys(n)
            parts = []
            for odd in range(2):
                vals = jnp.where(row_k == 0, zero, kv if odd else swapped)
                ext = jnp.where((lane_k >= HEAD_DIM) if odd else (lane_k < HEAD_DIM), vals, one)
                parts.append(dot(eb[2 * n + odd], ext))
            low = lane_q < HEAD_DIM
            num = jnp.where(low, parts[0], parts[1])
            den = pltpu.roll(jnp.where(low, parts[1], parts[0]), HEAD_DIM, 1)
            res = (num / den).astype(bf16)
            blocks.append(jnp.concatenate([res[:QB], res[QB:]], axis=1))
        win = jnp.concatenate(blocks, axis=0)

        @pl.when(off == 0)
        def _():
            wall[0] = win

        @pl.when(off > 0)
        def _():
            wrow[off] = win
            rows_send(wrow, wall, ws, wr, off)

    @pl.loop(0, NF)
    def _(i):
        off = jnp.where(i == 0, 2, jnp.where(i == 1, NF - 1, jnp.where(i == 2, 1, 0)))
        b = lax.rem(f + off, NF)

        with scope("o_state"):
            @pl.when(b != yy)
            def _():
                got(state_in.at[b], qr.at[b])

            @pl.when(b == yy)
            def _():
                got(state_in.at[b, pl.ds(0, NZ - 1)], qr.at[b])

        gate = gates[b].astype(f32)
        o = oacc[b] + dot(reach[b], state_in[b].reshape(LK, GLA_VALUE))
        scaled = o * lax.rsqrt(jnp.mean(o * o, axis=1, keepdims=True) + norm_epsilon)
        lin = (scaled * gain[...] * (gate / (1.0 + jnp.exp(-gate)))).astype(bf16)

        @pl.when(off == 0)
        def _():
            lall[0] = lin

        @pl.when(off > 0)
        def _():
            lrow[off] = lin
            rows_send(lrow, lall, ls, lr, off)

    with scope("n_ow"):
        relay_arrive(2)
        got(OW.at[pl.ds(1, 2), pl.ds(ZR, XR), cols_t], orr.at[2])
        core_send(3, ow_x)
    with scope("n_ring4"):
        ring_step(4)

    with scope("p_ow"):
        got(whole(2, NY), drcv.at[2])
        got(ow_x, drcv.at[3])
        got(ring_all, drcv.at[4])
    with scope("p_wrow"):
        got(wall.at[pl.ds(1, NF - 1)], wr.at[0])

    chunk = 512

    def out_copy(c):
        cs = pl.ds(c * chunk, chunk)
        return pltpu.make_async_copy(obuf.at[:, cs], out.at[:, cs], lsem.at[c])

    def project(lo, hi, rows_of, init):
        lhs = jnp.concatenate([rows_of[n] for n in range(NF)], axis=1)
        for c in range(depth // chunk):
            cs = slice(c * chunk, (c + 1) * chunk)
            y = dot(lhs, OW[:, lo:hi, cs].reshape(-1, chunk))
            if init:
                acc[:, cs] = y
            else:
                obuf[:, cs] = (acc[:, cs] + y).astype(bf16)
                out_copy(c).start()

    with scope("q_proj1"):
        project(lin_rows, orows, wall, True)
    with scope("r_lrow"):
        got(lall.at[pl.ds(1, NF - 1)], lr.at[0])
    with scope("s_proj2"):
        project(0, lin_rows, lall, False)

    with scope("t_end"):
        gone(toks.at[pl.ds(0, NF - 1)], ts.at[0])
        gone(ow_x, os.at[0])
        gone(slices(2), xs.at[0])
        gone(slices(3), xs.at[1])
        gone(OW.at[others, ow_rows(3, 0, 1), pl.ds(0, (NY - 1) * tile_c)], ys.at[3])
        gone(OW.at[others, ow_rows(3, 0, NZ - 1), cols_t], zs.at[3])
        gone(ring_all, dsnd.at[4])
        gone(wrow.at[pl.ds(1, NF - 1)], ws.at[0])
        gone(lrow.at[pl.ds(1, NF - 1)], ls.at[0])
        for g in range(3):
            gone(box(g, 0, NZ - 1, 0), zs.at[g])
            gone(whole(g, 3), ys.at[g])
            gone(whole(g, NY), dsnd.at[g])
        gone(ow_x, dsnd.at[3])
        gone(arr.at[pl.ds(0, NS - 1)], asnd.at[0])
        gone(pre.at[pl.ds(0, NS - 1)], qs.at[0])

        @pl.when(sp < NS - 1)
        def _():
            gone(kvbuf.at[:, pl.ds(0, WINDOW)], hs.at[0])

        for c in range(depth // chunk):
            out_copy(c).wait()


def shards(
    NS, NF, NT,
    tokens, linear_query, linear_key, linear_decay, linear_value, linear_gate, decay_bias,
    norm_gain, window_query, window_key, window_value, sink_logit, linear_output, window_output,
):
    _, length, depth = tokens.shape
    kb = linear_query.shape[0]
    NZ = NS // NY
    levels = []
    h = 1
    while h < length:
        levels.append(h)
        h *= 2
    vm = pltpu.VMEM
    dma = pltpu.SemaphoreType.DMA
    kv_width = window_key.shape[1] + window_value.shape[1]
    width1 = 3 * GLA_KEY + GLA_VALUE + kv_width
    width2 = window_query.shape[1] + GLA_VALUE
    anyspec = pl.BlockSpec(memory_space=pl.ANY)
    vspec = pl.BlockSpec(memory_space=vm)
    result = pl.pallas_call(
        functools.partial(kernel, NS, NF, NT, tuple(levels)),
        out_shape=jax.ShapeDtypeStruct((length, depth), bf16),
        in_specs=[anyspec] * 9 + [vspec] * 5,
        out_specs=anyspec,
        scratch_shapes=[
            vm((NF, length, depth), bf16),
            vm((NZ, NY, NT, kb, width1), bf16),
            vm((NZ, NY, NT, kb, width2), bf16),
            vm((NF, linear_output.shape[0] + window_output.shape[0], depth), bf16),
            vm((len(levels) + 2, length, length), bf16),
            vm((NF, length, 2 * GLA_KEY), bf16),
            vm((NF, length, GLA_KEY), bf16),
            vm((NF, length, GLA_VALUE), bf16),
            vm((NF, length, GLA_KEY), bf16),
            vm((NF, length + WINDOW, kv_width), bf16),
            vm((NF, NZ, GLA_KEY // NZ, GLA_VALUE + 128), bf16),
            vm((NS, GLA_KEY // NZ, GLA_VALUE + 128), bf16),
            vm((NS, GLA_KEY // NZ, GLA_VALUE), bf16),
            vm((NF, NZ, GLA_KEY // NZ, GLA_VALUE), bf16),
            vm((NF, length, GLA_VALUE), bf16),
            vm((NF, length, window_query.shape[1]), bf16),
            vm((NF, length, GLA_VALUE), bf16),
            vm((NF, length, window_query.shape[1]), bf16),
            vm((NF, length, GLA_VALUE), f32),
            vm((NF, length, GLA_KEY), bf16),
            vm((NF, length, GLA_VALUE), bf16),
            vm((length, depth), f32),
            vm((length, depth), bf16),
            vm((6, 128, 192), f32),
            vm((6, 128, 192), bf16),
            dma((9,)),
            dma((4,)), dma((NZ // 2 + 2,)), dma((2, NZ // 2)),
            dma((4,)), dma((2, NZ // 2 + 4)),
            dma((3,)),
            dma((5,)), dma((5,)),
            dma((1,)), dma((5,)),
            dma((1,)), dma((NF,)),
            dma((1,)), dma((1,)),
            dma((1,)), dma((NF,)),
            dma((1,)), dma((1,)),
            dma((1,)), dma((1,)),
            dma((2,)), dma((2,)),
            dma((1,)), dma((3,)),
        ],
        compiler_params=pltpu.CompilerParams(
            collective_id=0, has_side_effects=True, vmem_limit_bytes=60 * 1024 * 1024),
        name="layer",
    )(tokens[0], linear_decay, linear_key, linear_value, linear_query, window_query, linear_gate,
      linear_output, window_output, window_key, window_value,
      decay_bias[None], norm_gain[None], sink_logit[None])
    return result[None]


def solution(mesh):
    shape = mesh.shape
    return jax.shard_map(
        functools.partial(shards, shape["sp"], shape["fs"], shape["tp"]),
        mesh=mesh,
        in_specs=(
            P(("fs", "tp"), "sp", None),
            P(("sp", "tp"), "fs"),
            P(("sp", "tp"), "fs"),
            P(("sp", "tp"), "fs"),
            P(("sp", "tp"), "fs"),
            P(("sp", "tp"), "fs"),
            P("fs"),
            P(),
            P(("sp", "tp"), "fs"),
            P(("sp", "tp"), "fs"),
            P(("sp", "tp"), "fs"),
            P("fs"),
            P("fs", None),
            P("fs", None),
        ),
        out_specs=P(("fs", "tp"), "sp", None),
        check_vma=False,
    )
```
